32 devices in a mesh: fs: 8 (over z, x), tp: 4 (over y, core).
Axes of the slice: x: 2, y: 2, z: 4, core: 2. Of those that a mesh axis runs over, the one named last changes fastest.
Arguments:
- inputs: bfloat16 [1024, 2048], P('fs', 'tp'), may hold values from -6 to 6
- query_grad: bfloat16 [1024, 1024], P('fs', 'tp'), may hold values from -6 to 6
- forget_grad: bfloat16 [1024, 1024], P('fs', 'tp'), may hold values from -6 to 6
- forget_pre: bfloat16 [1024, 1024], P('fs', 'tp'), may hold values from -8 to 8
- lower_bound: float32 [1024], P('tp'), may hold values from 0.1 to 0.9
- query_weight: float32 [2048, 1024], P('fs', 'tp'), may hold values from -0.125 to 0.125
- forget_weight: float32 [2048, 1024], P('fs', 'tp'), may hold values from -0.125 to 0.125
- query_moment: float32 [2048, 1024], P('fs', 'tp'), may hold values from -6 to 6
- forget_moment: float32 [2048, 1024], P('fs', 'tp'), may hold values from -6 to 6
- query_rows: float32 [2048, 2048], P('fs'), may hold values from -0.6 to 0.6
- forget_rows: float32 [2048, 2048], P('fs'), may hold values from -0.6 to 0.6
- query_cols: float32 [8, 128, 128], P('tp'), may hold values from -0.6 to 0.6
- forget_cols: float32 [8, 128, 128], P('tp'), may hold values from -0.6 to 0.6
- query_row_root: bfloat16 [2048, 2048], P('fs'), may hold values from -2 to 2, as said below
- forget_row_root: bfloat16 [2048, 2048], P('fs'), may hold values from -2 to 2, as said below
- query_col_root: bfloat16 [8, 128, 128], P('tp'), may hold values from -2 to 2, as said below
- forget_col_root: bfloat16 [8, 128, 128], P('tp'), may hold values from -2 to 2, as said below
Outputs:
- query_master: float32 [2048, 1024], P('fs', 'tp')
- forget_master: float32 [2048, 1024], P('fs', 'tp')
- query_copy: bfloat16 [2048, 1024], P('fs', 'tp')
- forget_copy: bfloat16 [2048, 1024], P('fs', 'tp')
- query_step: float32 [2048, 1024], P('fs', 'tp')
- forget_step: float32 [2048, 1024], P('fs', 'tp')
- query_moment_next: float32 [2048, 1024], P('fs', 'tp')
- forget_moment_next: float32 [2048, 1024], P('fs', 'tp')
- query_rows_next: float32 [2048, 2048], P('fs')
- forget_rows_next: float32 [2048, 2048], P('fs')
- query_cols_next: float32 [8, 128, 128], P('tp')
- forget_cols_next: float32 [8, 128, 128], P('tp')
The draws below stay inside these ranges and needn't reach their ends.
Inputs may be any that keep to these rules, and one draw needn't show every extreme that they name: `query_row_root`: diagonal entries 0.5 to 1.5, the others of order 2048 ** -0.5. `forget_row_root`: diagonal entries 0.5 to 1.5, the others of order 2048 ** -0.5. `query_col_root`: diagonal entries 0.5 to 1.5, the others of order 128 ** -0.5. `forget_col_root`: diagonal entries 0.5 to 1.5, the others of order 128 ** -0.5.
All inputs are finite; a program needn't handle non-finite values.
Results may differ from the reference program's by a relative error of at most 0.005.
Values may be sent and summed in bfloat16 or wider, within the bound.
A program may use at most 64 MiB of HBM per device.

```python
import jax
import jax.numpy as jnp
from jax import lax

D = 2048
HW = 1024
HEAD = 128
TOKENS = 1024
HEADS = 8


def root_matrix(key, shape):
    order = shape[-1]
    diag_key, spread_key = jax.random.split(key)
    spread = jnp.clip(jax.random.normal(spread_key, shape, jnp.float32), -4.0, 4.0) * order ** (-0.5)
    diagonal = jax.random.uniform(diag_key, shape[:-1], jnp.float32, 0.5, 1.5)
    unit_eye = jnp.eye(order, dtype=jnp.float32)
    return (spread * (1.0 - unit_eye) + diagonal[..., None] * unit_eye).astype(jnp.bfloat16)


def draw_query_row_root(key, part):
    return root_matrix(jax.random.fold_in(key, 11), (D, D))


def draw_forget_row_root(key, part):
    return root_matrix(jax.random.fold_in(key, 23), (D, D))


def draw_query_col_root(key, part):
    return root_matrix(jax.random.fold_in(key, 37), (HEADS, HEAD, HEAD))


def draw_forget_col_root(key, part):
    return root_matrix(jax.random.fold_in(key, 41), (HEADS, HEAD, HEAD))


def raised(entries, own_key, source, target, parts, factor):
    owner, partner = [(jnp.arange(entries.shape[dim]) // (entries.shape[dim] // parts)).reshape([-1 if axis == dim else 1 for axis in range(entries.ndim)]) for dim in (source, target)]
    chosen = jax.random.permutation(own_key, parts)[partner]
    strong = (owner == chosen) | (owner == (partner + parts // 2) % parts)
    return jnp.where(strong, factor * entries, entries)


def steps_of(rng, shape, shards, low, high):
    factor_of, own = 1.0, jax.random.fold_in(rng, 6)
    for dim, shards_of in shards:
        steps = jnp.exp(jax.random.uniform(jax.random.fold_in(own, dim), (shards_of,), jnp.float32, low / len(shards), high / len(shards)))
        factor_of = factor_of * jnp.repeat(steps, shape[dim] // shards_of).reshape([-1 if axis == dim else 1 for axis in range(len(shape))])
    return factor_of


def gaussian(rng, extent, deviation, bound, cuts=(), kind=jnp.bfloat16):
    array = jax.random.normal(rng, extent, jnp.float32) * deviation
    if len(cuts) > 0:
        array = steps_of(rng, extent, cuts, -0.22, 0.18) * array
    return jnp.clip(array, min=-bound, max=bound).astype(kind)


def bell_draw_with(key, extent, deviation, limit, shards, heavy, held_as=jnp.bfloat16):
    drawn = deviation * jax.random.normal(key, extent, jnp.float32)
    if shards:
        drawn = drawn * steps_of(key, extent, shards, -0.22, 0.18)
    return jnp.clip(raised(drawn, jax.random.fold_in(key, 3), *heavy), -limit, limit).astype(held_as)


def setup_inputs(seed: int = 0) -> dict:
    key_list = jax.random.split(jax.random.key(seed), 18)
    inputs = bell_draw_with(key_list[0], (TOKENS, D), 1.0, 6.0, ((0, 8), (1, 4)), (0, 1, 8, 2.0))
    query_grad = gaussian(key_list[1], (TOKENS, HW), 1.0, 6.0, ((0, 8), (1, 4)))
    forget_grad = gaussian(key_list[2], (TOKENS, HW), 1.0, 6.0, ((0, 8), (1, 4)))
    forget_pre = gaussian(key_list[3], (TOKENS, HW), 2.0, 8.0, ((0, 8), (1, 4)))
    lower_bound = jnp.clip(0.1 + 0.79999997 * jax.random.uniform(key_list[4], (HW,), jnp.float32) ** steps_of(key_list[4], (HW,), ((0, 4),), -0.2, 0.2), 0.1, 0.9)
    query_weight = gaussian(key_list[5], (D, HW), D ** -0.5, 0.125, ((0, 8), (1, 4)), jnp.float32)
    forget_weight = gaussian(key_list[6], (D, HW), D ** -0.5, 0.125, ((0, 8), (1, 4)), jnp.float32)
    query_moment = gaussian(key_list[7], (D, HW), 1.0, 6.0, ((0, 8), (1, 4)), jnp.float32)
    forget_moment = gaussian(key_list[8], (D, HW), 1.0, 6.0, ((0, 8), (1, 4)), jnp.float32)
    query_rows = gaussian(key_list[9], (D, D), 0.1, 0.6, ((0, 8),), jnp.float32)
    forget_rows = gaussian(key_list[10], (D, D), 0.1, 0.6, ((0, 8),), jnp.float32)
    query_cols = gaussian(key_list[11], (HEADS, HEAD, HEAD), 0.1, 0.6, ((0, 4),), jnp.float32)
    forget_cols = gaussian(key_list[12], (HEADS, HEAD, HEAD), 0.1, 0.6, ((0, 4),), jnp.float32)
    query_row_root = draw_query_row_root(jax.random.fold_in(key_list[17], 71), 0)
    forget_row_root = draw_forget_row_root(jax.random.fold_in(key_list[17], 71), 0)
    query_col_root = draw_query_col_root(jax.random.fold_in(key_list[17], 71), 0)
    forget_col_root = draw_forget_col_root(jax.random.fold_in(key_list[17], 71), 0)
    return dict(inputs=inputs, query_grad=query_grad, forget_grad=forget_grad, forget_pre=forget_pre, lower_bound=lower_bound, query_weight=query_weight, forget_weight=forget_weight, query_moment=query_moment, forget_moment=forget_moment, query_rows=query_rows, forget_rows=forget_rows, query_cols=query_cols, forget_cols=forget_cols, query_row_root=query_row_root, forget_row_root=forget_row_root, query_col_root=query_col_root, forget_col_root=forget_col_root)


stat_decay = 0.9
moment_decay = 0.9
learn_rate = 0.02
highest = lax.Precision.HIGHEST

def finish(gradient, weight, moment, rows, cols, row_root, col_root):
    square = jnp.sum(gradient * gradient)
    norm_scale = jnp.sqrt(D * HW / (square + 1.0))
    scaled = gradient * norm_scale
    rows_next = stat_decay * rows + (1.0 - stat_decay) / HW * jnp.dot(scaled, scaled.T, precision=highest)
    by_head = scaled.reshape(D, HEADS, HEAD)
    cols_next = stat_decay * cols + (1.0 - stat_decay) / D * jnp.einsum('rhi,rhj->hij', by_head, by_head, precision=highest)
    left_sum = jnp.dot(row_root.astype(jnp.float32), gradient, precision=highest)
    precond = norm_scale * jnp.einsum('rhi,hij->rhj', left_sum.reshape(D, HEADS, HEAD), col_root.astype(jnp.float32), precision=highest).reshape(D, HW)
    moment_next = moment_decay * moment + (1.0 - moment_decay) * precond
    update_step = moment_decay * moment_next + (1.0 - moment_decay) * precond
    master = weight - learn_rate * update_step
    return (master, master.astype(jnp.bfloat16), update_step, moment_next, rows_next, cols_next)

def reference(inputs, query_grad, forget_grad, forget_pre, lower_bound, query_weight, forget_weight, query_moment, forget_moment, query_rows, forget_rows, query_cols, forget_cols, query_row_root, forget_row_root, query_col_root, forget_col_root):
    sigma_gate = jax.nn.sigmoid(forget_pre.astype(jnp.float32))
    forget_cot = (forget_grad.astype(jnp.float32) * (1.0 - lower_bound) * sigma_gate * (1.0 - sigma_gate)).astype(jnp.bfloat16)
    query_gradient = jnp.dot(inputs.T, query_grad, preferred_element_type=jnp.float32)
    forget_gradient = jnp.dot(inputs.T, forget_cot, preferred_element_type=jnp.float32)
    query_out = finish(query_gradient, query_weight, query_moment, query_rows, query_cols, query_row_root, query_col_root)
    forget_out = finish(forget_gradient, forget_weight, forget_moment, forget_rows, forget_cols, forget_row_root, forget_col_root)
    return (query_out[0], forget_out[0], query_out[1], forget_out[1], query_out[2], forget_out[2], query_out[3], forget_out[3], query_out[4], forget_out[4], query_out[5], forget_out[5])
```

```python
import functools

import jax
import jax.numpy as jnp
from jax import lax
from jax.experimental import pallas as pl
from jax.experimental.pallas import tpu as pltpu
from jax.sharding import PartitionSpec as P

D = 2048
HW = 1024
HEAD = 128


stat_decay = 0.9
moment_decay = 0.9
learn_rate = 0.02
highest = lax.Precision.HIGHEST
MESH = pl.DeviceIdType.MESH


def fold_one(carry_state, shard_piece, offset, root_mine, grad_mine):
    left_sum, outer_rows, column_total = carry_state
    row_count, col_width = shard_piece.shape
    left_sum = left_sum + jnp.dot(root_mine, shard_piece, precision=highest)
    outer_piece = lax.dot_general(
        grad_mine, shard_piece, (((1,), (1,)), ((), ())), precision=highest
    )
    outer_rows = lax.dynamic_update_slice_in_dim(outer_rows, outer_piece, offset, 1)
    by_head = shard_piece.reshape(row_count, col_width // HEAD, HEAD)
    column_total = column_total + jnp.einsum("rhi,rhj->hij", by_head, by_head, precision=highest)
    return (left_sum, outer_rows, column_total)


def finish(weight, moment, rows, cols, col_root, left_sum, outer_rows, column_total, square):
    norm_scale = jnp.sqrt(D * HW / (square + 1.0))
    scale_twice = norm_scale * norm_scale
    rows_next = stat_decay * rows + (1.0 - stat_decay) / HW * scale_twice * outer_rows
    cols_next = stat_decay * cols + (1.0 - stat_decay) / D * scale_twice * column_total
    shard_rows, col_width = left_sum.shape
    shaped = left_sum.reshape(shard_rows, col_width // HEAD, HEAD)
    precond = norm_scale * jnp.einsum(
        "rhi,hij->rhj", shaped, col_root.astype(jnp.float32), precision=highest
    ).reshape(shard_rows, col_width)
    moment_next = moment_decay * moment + (1.0 - moment_decay) * precond
    update_step = moment_decay * moment_next + (1.0 - moment_decay) * precond
    master = weight - learn_rate * update_step
    return (master, master.astype(jnp.bfloat16), update_step, moment_next, rows_next, cols_next)


def reduce_plan(
    inputs,
    query_grad,
    forget_grad,
    forget_pre,
    lower_bound,
    query_weight,
    forget_weight,
    query_moment,
    forget_moment,
    query_rows,
    forget_rows,
    query_cols,
    forget_cols,
    query_row_root,
    forget_row_root,
    query_col_root,
    forget_col_root,
):
    sigma_gate = jax.nn.sigmoid(forget_pre.astype(jnp.float32))
    forget_cot = (
        forget_grad.astype(jnp.float32) * (1.0 - lower_bound) * sigma_gate * (1.0 - sigma_gate)
    ).astype(jnp.bfloat16)
    gathered = lax.all_gather(inputs, "tp", axis=1, tiled=True)
    shard_rows, col_width = query_weight.shape
    heads_here = col_width // HEAD
    row_roots = (query_row_root.astype(jnp.float32), forget_row_root.astype(jnp.float32))
    empty = (
        jnp.zeros((shard_rows, col_width), jnp.float32),
        jnp.zeros((shard_rows, D), jnp.float32),
        jnp.zeros((heads_here, HEAD, HEAD), jnp.float32),
    )
    joined = jnp.concatenate([query_grad, forget_cot], axis=1)
    summed = lax.psum_scatter(
        lax.dot_general(
            gathered, joined, (((0,), (0,)), ((), ())), preferred_element_type=jnp.float32
        ),
        "fs",
        scatter_dimension=0,
        tiled=True,
    )
    gradients = (summed[:, :col_width], summed[:, col_width:])
    offset = jnp.int32(0)
    results = (
        fold_one(
            empty,
            lax.all_gather(gradients[0].astype(jnp.bfloat16), "fs", axis=0, tiled=True).astype(
                jnp.float32
            ),
            offset,
            row_roots[0],
            gradients[0],
        ),
        fold_one(
            empty,
            lax.all_gather(gradients[1].astype(jnp.bfloat16), "fs", axis=0, tiled=True).astype(
                jnp.float32
            ),
            offset,
            row_roots[1],
            gradients[1],
        ),
    )
    query_trace = jnp.sum(jnp.diagonal(results[0][2], axis1=1, axis2=2))
    forget_trace = jnp.sum(jnp.diagonal(results[1][2], axis1=1, axis2=2))
    query_outer, forget_outer, query_square, forget_square = (
        lax.psum(results[0][1].astype(jnp.bfloat16), "tp").astype(jnp.float32),
        lax.psum(results[1][1].astype(jnp.bfloat16), "tp").astype(jnp.float32),
        lax.psum(query_trace.astype(jnp.bfloat16), "tp").astype(jnp.float32),
        lax.psum(forget_trace.astype(jnp.bfloat16), "tp").astype(jnp.float32),
    )
    query_out = finish(
        query_weight,
        query_moment,
        query_rows,
        query_cols,
        query_col_root,
        results[0][0],
        query_outer,
        results[0][2],
        query_square,
    )
    forget_out = finish(
        forget_weight,
        forget_moment,
        forget_rows,
        forget_cols,
        forget_col_root,
        results[1][0],
        forget_outer,
        results[1][2],
        forget_square,
    )
    return (
        query_out[0],
        forget_out[0],
        query_out[1],
        forget_out[1],
        query_out[2],
        forget_out[2],
        query_out[3],
        forget_out[3],
        query_out[4],
        forget_out[4],
        query_out[5],
        forget_out[5],
    )


def to_bf16(value):
    return value.astype(jnp.bfloat16)


def wide_dot(left, right, dims):
    return lax.dot_general(left, right, (dims, ((), ())), preferred_element_type=jnp.float32)


LAYERS = "ABCD"
ACROSS = {"p": {"c": "p", "p": "c", "s": "d", "d": "s"}, "s": {"c": "s", "s": "c", "p": "d", "d": "p"}}
ROUTES = {
    "Ac": ("b", "m", "p", "s"),
    "Bc": ("m", "s"),
    "Cc": ("n", "p", "s"),
    "Dc": ("n", "p", "s"),
    "Ap": ("s", "b"),
    "Cp": ("s",),
    "Dp": ("s",),
    "Ad": ("b",),
}
PROGRAM = (
    "o0", "o1", "w0Ap", "w0As", "w0Bc", "w1Ap", "w1As", "w1Bc", "w0Cc", "w0Bp", "w0Ad", "w0Bs",
    "w1Cc", "w0Cp", "w0Cs", "w1Bp", "w0Dc", "w1Ad", "TA", "w1Bs", "o2", "w1Cp", "w1Dc", "w0Bd",
    "w0Dp", "o3", "w2Ap", "w1Cs", "w0Cd", "w1Bd", "TB", "w1Dp", "w2Bc", "w0Ds", "w2Cc", "w2As",
    "w3Ap", "w1Cd", "TC", "w1Ds", "w2Bp", "w3Bc", "w2Cp", "w2Dc", "w0Dd", "w2Ad", "w3Cc", "w3As",
    "w1Dd", "TD", "w2Bs", "M20AB", "OAB", "w2Dp", "w3Bp", "w3Dc", "w2Cs", "M20C", "OC", "w3Cp",
    "w3Ad", "w2Bd", "M21AB", "w3Bs", "M30AB", "w2Ds", "M20D", "OD", "L", "Q", "w3Dp", "w2Cd",
    "M21C", "w3Cs", "M30C", "w3Bd", "M31AB", "w2Dd", "M21D", "S01", "w3Ds", "M30D", "S22", "P",
    "w3Cd", "M31C", "w3Dd", "M31D", "S33",
)


def relay_kernel(
    x_hbm, q_hbm, g_hbm, pre_hbm, bound_ref, rq_hbm, rf_hbm, cq_hbm, cf_hbm,
    s_ref, pre_ref, k_ref,
    xs, gs, go, xt, acc, oacc, grad, ograd, sacc, norms, roots, col_roots, raw,
    own_sem, send_sem, x_sem, g_sem, o_sem, swap_sem,
):
    shards, parts, block, span = xs.shape
    width = go.shape[2]
    features = xt.shape[1]
    chunk = s_ref.shape[1]
    heads = width // HEAD
    f32 = jnp.float32
    fs = lax.axis_index("fs")
    tp = lax.axis_index("tp")
    z, px = lax.div(fs, 2), lax.rem(fs, 2)
    py, pc = lax.div(tp, 2), lax.rem(tp, 2)
    pair = z + 1 - 2 * lax.rem(z, 2)
    low = z < 2
    near = jnp.where(low, 2, 1)
    layer = {"A": z, "B": pair, "C": near, "D": jnp.where(low, 3, 0)}
    middle = jnp.logical_and(z > 0, z < 3)
    flips = {"c": (0, 0), "p": (1 - pc, pc), "s": (pc, 1 - pc), "d": (1, 1)}

    def column(who):
        flip_x, flip_y = flips[who]
        return px + flip_x - 2 * px * flip_x, py + flip_y - 2 * py * flip_y

    def device(link):
        if link in ("b", "n"):
            return (2 * pair + px, tp)
        if link == "m":
            return (2 * near + px, tp)
        if link == "core":
            return (fs, tp + 1 - 2 * pc)
        x, y = column(link)
        return (2 * z + x, 2 * y + pc)

    beside = {link: device(link) for link in ("b", "n", "m", "p", "s", "core")}
    conds = {"n": middle, "m": middle}

    def guarded(cond, action):
        if cond is None:
            action()
        else:
            pl.when(cond)(action)

    barrier = pltpu.get_barrier_semaphore()

    def greet(name):
        pl.semaphore_signal(barrier, inc=1, device_id=beside[name], device_id_type=MESH)

    for name in ("b", "p", "s", "core"):
        greet(name)
    guarded(middle, lambda: greet("m"))
    loads = [
        pltpu.make_async_copy(source, target, own_sem.at[number])
        for number, (source, target) in enumerate(
            (
                (x_hbm, xs.at[fs, tp]),
                (q_hbm, raw.at[0]),
                (g_hbm, raw.at[1]),
                (pre_hbm, raw.at[2]),
                (rq_hbm, roots.at[0]),
                (rf_hbm, roots.at[1]),
                (cq_hbm, col_roots.at[0]),
                (cf_hbm, col_roots.at[1]),
            )
        )
    ]
    for load in loads:
        load.start()
    for load in loads[1:4]:
        load.wait()
    sigma_gate = jax.nn.sigmoid(raw[2].astype(f32))
    cot = to_bf16(
        raw[1].astype(f32) * (1.0 - bound_ref[...]) * sigma_gate * (1.0 - sigma_gate)
    )

    @pl.when(pc == 0)
    def _():
        gs[fs, py, 0] = raw[0]
        go[fs] = cot

    @pl.when(pc == 1)
    def _():
        gs[fs, py, 1] = cot
        go[fs] = raw[0]

    loads[0].wait()
    pl.semaphore_wait(barrier, 4 + jnp.where(middle, 1, 0))

    half_rows = block // 2
    pending = []
    dones = []

    def halves(phase):
        return 1 - pc if phase == 2 else pc

    def piece(phase, name):
        x, y = column(name[1])
        shard = 2 * layer[name[0]] + x
        if phase < 2:
            rows = pl.ds(phase * half_rows, half_rows)
            part = 2 * y + pc
            return xs.at[shard, part, rows], x_sem.at[phase, shard, part]
        return gs.at[shard, y, halves(phase)], g_sem.at[phase - 2, shard, y]

    def start(src, dst, sem, link, cond=None):
        number = len(pending)

        def build():
            return pltpu.make_async_remote_copy(
                src_ref=src, dst_ref=dst, send_sem=send_sem.at[number], recv_sem=sem,
                device_id=beside[link], device_id_type=MESH,
            )

        guarded(cond, lambda: build().start())
        pending.append((cond, build))

    def landed(ref, sem):
        pltpu.make_async_remote_copy(
            src_ref=ref, dst_ref=ref, send_sem=send_sem.at[0], recv_sem=sem,
            device_id=beside["core"], device_id_type=MESH,
        ).wait_recv()

    def forward(phase, name):
        here, sem = piece(phase, name)
        for link in ROUTES.get(name, ()):
            start(here, here, sem, link, conds.get(link))
        if phase < 2:
            start(here, here, sem, "core")
        if phase == 2 and name != "Ac" and name[1] != "d":
            cond = {"c": None, "p": pc == 0, "s": pc == 1}[name[1]]
            shard = 2 * layer[name[0]] + column(name[1])[0]
            start(here, go.at[shard], o_sem.at[shard], "core", cond)

    start(go.at[fs], gs.at[fs, py, pc], g_sem.at[0, fs, py], "core")

    def from_core(label):
        for phase in range(2):
            for x in range(2):
                for y in range(2):
                    shard, part = 2 * layer[label] + x, 2 * y + 1 - pc
                    rows = pl.ds(phase * half_rows, half_rows)
                    landed(xs.at[shard, part, rows], x_sem.at[phase, shard, part])

    def transpose(label):
        at = LAYERS.index(label)
        for x in range(2):
            for part in range(parts):
                turned = xs[2 * layer[label] + x, part].T
                xt[at, part * span : (part + 1) * span, x * block : (x + 1) * block] = turned

    squares = []
    tile = 512
    steps = features // tile

    def multiply(labels, block_of, into, out, lanes, first, final):
        def body(step, total):
            rows = pl.ds(pl.multiple_of(step * tile, tile), tile)
            value = None
            for label in labels:
                product = wide_dot(xt[LAYERS.index(label), rows, :], block_of(label), ((1,), (0,)))
                value = product if value is None else value + product
            if not first:
                value = value + into[rows, :]
            if final:
                out[rows, lanes] = to_bf16(value)
                squared = (value * value).reshape(tile // 8, 8, width)
                return total + jnp.sum(squared, axis=0)
            into[rows, :] = value
            return total

        total = lax.fori_loop(0, steps, body, jnp.zeros((8, width), f32))
        if final:
            squares.append(total)

    def own_block(phase, far):
        y = 1 - py if far else py

        def block_of(label):
            both = pl.ds(2 * layer[label], 2)
            return gs[both, y, halves(phase)].reshape(2 * block, width)

        return block_of

    def other_block(label):
        return go[pl.ds(2 * layer[label], 2)].reshape(2 * block, width)

    mine = pl.ds(pl.multiple_of(fs * chunk, chunk), chunk)
    size = float(features * grad.shape[1])

    def outer_step(lanes, first, final):
        wide = 2 * chunk
        if final:
            square = jnp.sum(squares[0], axis=(0, 1), keepdims=True)
            for more in squares[1:]:
                square = square + jnp.sum(more, axis=(0, 1), keepdims=True)
            norms[0] = jnp.broadcast_to(square, norms.shape[1:])
            scale = (1.0 - stat_decay) / grad.shape[1] * (size / (square + 1.0))
            swap_norm = pltpu.make_async_remote_copy(
                src_ref=norms.at[0], dst_ref=norms.at[1],
                send_sem=swap_sem.at[0], recv_sem=swap_sem.at[1],
                device_id=beside["core"], device_id_type=MESH,
            )
        left = grad[mine, lanes]
        for step in range(features // wide):
            rows = slice(step * wide, (step + 1) * wide)
            product = wide_dot(left, grad[rows, lanes], ((1,), (1,)))
            if not first:
                product = product + sacc[:, rows]
            if not final:
                sacc[:, rows] = product
                continue
            s_ref[pc, :, rows] = to_bf16(product * scale)
            if step == 0:
                swap_norm.start()
                dones.append(swap_norm)
            else:
                send_outer(step - 1)
        if final:
            send_outer(features // wide - 1)

    def outer_copy(which, step):
        rows = pl.ds(step * 2 * chunk, 2 * chunk)
        return pltpu.make_async_remote_copy(
            src_ref=s_ref.at[which, :, rows], dst_ref=s_ref.at[which, :, rows],
            send_sem=swap_sem.at[2 + step], recv_sem=swap_sem.at[6 + step],
            device_id=beside["core"], device_id_type=MESH,
        )

    def send_outer(step):
        outer_copy(pc, step).start()
        dones.append(step)

    def products(which, source, lanes):
        left = wide_dot(roots[which], source[:, lanes], ((1,), (0,)))

        def body(step, sums):
            rows = pl.ds(pl.multiple_of(step * chunk, chunk), chunk)
            outs = []
            for head in range(heads):
                start_lane = lanes.start + head * HEAD
                part = source[rows, start_lane : start_lane + HEAD]
                outs.append(sums[head] + wide_dot(part, part, ((0,), (0,))))
            return tuple(outs)

        sums = lax.fori_loop(
            0, features // chunk, body, tuple(jnp.zeros((HEAD, HEAD), f32) for _ in range(heads))
        )
        for head in range(heads):
            at = slice(head * HEAD, (head + 1) * HEAD)
            k_ref[which, head] = sums[head]
            pre_ref[which, :, at] = wide_dot(
                to_bf16(left[:, at]), col_roots[which, head], ((1,), (0,))
            )

    everything = slice(0, width)
    for op in PROGRAM:
        kind, rest = op[0], op[1:]
        if kind == "o":
            phase = int(rest)
            if phase == 2:
                landed(*piece(phase, "Ac"))
            forward(phase, "Ac")
        elif kind == "w":
            phase, name = int(rest[0]), rest[1:]
            landed(*piece(phase, name))
            forward(phase, name)
        elif kind == "T":
            from_core(rest)
            transpose(rest)
        elif kind == "M":
            phase, far, labels = int(rest[0]), int(rest[1]), rest[2:]
            at = 2 * (phase - 2) + far
            lanes = slice(at * width, (at + 1) * width)
            multiply(
                labels, own_block(phase, far), acc.at[at], grad, lanes,
                labels[0] == "A", labels[-1] == "D",
            )
        elif kind == "O":
            for label in rest:
                for x in range(2):
                    shard = 2 * layer[label] + x
                    if label == "A":
                        @pl.when(px != x)
                        def _():
                            landed(go.at[shard], o_sem.at[shard])
                    else:
                        landed(go.at[shard], o_sem.at[shard])
            multiply(
                rest, other_block, oacc, ograd, everything, rest[0] == "A", rest[-1] == "D"
            )
            if rest[-1] == "D":
                squares.pop()
        elif kind == "S":
            first, last = int(rest[0]), int(rest[1])
            outer_step(slice(first * width, (last + 1) * width), first == 0, last == 3)
        elif kind == "L":
            for load in loads[4:]:
                load.wait()
        elif kind == "P":
            products(pc, grad, slice(2 * width, 3 * width))
        elif kind == "Q":
            products(1 - pc, ograd, everything)

    dones[0].wait()
    mine_sum, their_sum = norms[0, 0:1, 0:1], norms[1, 0:1, 0:1]
    sums = (
        jnp.where(pc == 0, mine_sum, their_sum),
        jnp.where(pc == 0, their_sum, mine_sum),
    )
    for which in range(2):
        scale_twice = size / (sums[which] + 1.0)
        pre_ref[which] = pre_ref[which] * jnp.sqrt(scale_twice)
        for head in range(heads):
            k_ref[which, head] = k_ref[which, head] * (
                (1.0 - stat_decay) / features * scale_twice
            )
    for step in dones[1:]:
        outer_copy(pc, step).wait_send()
        outer_copy(1 - pc, step).wait_recv()
    for cond, build in pending:
        guarded(cond, lambda build=build: build().wait_send())


def relayed_products(
    x, query_grad, forget_grad, forget_pre, lower_bound,
    query_root, forget_root, query_col_root, forget_col_root,
):
    shards, parts = lax.axis_size("fs"), lax.axis_size("tp")
    block, span = x.shape
    width = query_grad.shape[1]
    chunk, features = query_root.shape
    bf16, f32 = jnp.bfloat16, jnp.float32
    heads = query_col_root.shape
    vmem = pl.BlockSpec(memory_space=pltpu.VMEM)
    hbm = pl.BlockSpec(memory_space=pltpu.HBM)
    return pl.pallas_call(
        relay_kernel,
        out_shape=[
            jax.ShapeDtypeStruct((2, chunk, features), bf16),
            jax.ShapeDtypeStruct((2, chunk, width), f32),
            jax.ShapeDtypeStruct((2,) + heads, f32),
        ],
        in_specs=[hbm] * 4 + [vmem] + [hbm] * 4,
        out_specs=[vmem] * 3,
        scratch_shapes=[
            pltpu.VMEM((shards, parts, block, span), bf16),
            pltpu.VMEM((shards, 2, 2, block, width), bf16),
            pltpu.VMEM((shards, block, width), bf16),
            pltpu.VMEM((shards // 2, features, 2 * block), bf16),
            pltpu.VMEM((4, features, width), f32),
            pltpu.VMEM((features, width), f32),
            pltpu.VMEM((features, parts * width), bf16),
            pltpu.VMEM((features, width), bf16),
            pltpu.VMEM((chunk, features), f32),
            pltpu.VMEM((2, 8, 128), f32),
            pltpu.VMEM((2, chunk, features), bf16),
            pltpu.VMEM((2,) + heads, bf16),
            pltpu.VMEM((3, block, width), bf16),
            pltpu.SemaphoreType.DMA((8,)),
            pltpu.SemaphoreType.DMA((128,)),
            pltpu.SemaphoreType.DMA((2, shards, parts)),
            pltpu.SemaphoreType.DMA((2, shards, 2)),
            pltpu.SemaphoreType.DMA((shards,)),
            pltpu.SemaphoreType.DMA((10,)),
        ],
        compiler_params=pltpu.CompilerParams(
            collective_id=0, has_side_effects=True, vmem_limit_bytes=61 * 1024 * 1024
        ),
    )(
        x, query_grad, forget_grad, forget_pre, lower_bound.reshape(1, -1),
        query_root, forget_root, query_col_root, forget_col_root,
    )


def finish_kernel(outer_ref, pre_ref, column_ref, *refs):
    weights, moments, rows, cols = (refs[2 * k : 2 * k + 2] for k in range(4))
    outs = refs[8:]
    for which in range(2):
        master_ref, copy_ref, step_ref, moment_ref, rows_ref, cols_ref = outs[which::2]
        precond = pre_ref[which]
        moment_next = moment_decay * moments[which][...] + (1.0 - moment_decay) * precond
        update_step = moment_decay * moment_next + (1.0 - moment_decay) * precond
        master = weights[which][...] - learn_rate * update_step
        master_ref[...] = master
        copy_ref[...] = to_bf16(master)
        step_ref[...] = update_step
        moment_ref[...] = moment_next
        rows_ref[...] = stat_decay * rows[which][...] + outer_ref[which].astype(jnp.float32)
        cols_ref[...] = stat_decay * cols[which][...] + column_ref[which]


def finished(outers, pres, columns, weights, moments, rows, cols):
    f32, bf16 = jnp.float32, jnp.bfloat16
    chunk, width = weights[0].shape
    features = rows[0].shape[1]
    heads = cols[0].shape
    steps = 2
    tile = chunk // steps
    narrow = pl.BlockSpec((tile, width), lambda i: (i, 0))
    wide = pl.BlockSpec((tile, features), lambda i: (i, 0))
    head = pl.BlockSpec((heads[0], heads[1] // steps, heads[2]), lambda i: (0, i, 0))
    both = pl.BlockSpec((2, tile, features), lambda i: (0, i, 0))
    both_narrow = pl.BlockSpec((2, tile, width), lambda i: (0, i, 0))
    both_head = pl.BlockSpec(
        (2, heads[0], heads[1] // steps, heads[2]), lambda i: (0, 0, i, 0)
    )
    flat = lambda kind: [jax.ShapeDtypeStruct((chunk, width), kind)] * 2
    return pl.pallas_call(
        finish_kernel,
        grid=(steps,),
        out_shape=flat(f32)
        + flat(bf16)
        + flat(f32)
        + flat(f32)
        + [jax.ShapeDtypeStruct((chunk, features), f32)] * 2
        + [jax.ShapeDtypeStruct(heads, f32)] * 2,
        in_specs=[both, both_narrow, both_head] + [narrow] * 4 + [wide] * 2 + [head] * 2,
        out_specs=[narrow] * 8 + [wide] * 2 + [head] * 2,
        compiler_params=pltpu.CompilerParams(vmem_limit_bytes=61 * 1024 * 1024),
    )(outers, pres, columns, *weights, *moments, *rows, *cols)


def gather_plan(
    inputs,
    query_grad,
    forget_grad,
    forget_pre,
    lower_bound,
    query_weight,
    forget_weight,
    query_moment,
    forget_moment,
    query_rows,
    forget_rows,
    query_cols,
    forget_cols,
    query_row_root,
    forget_row_root,
    query_col_root,
    forget_col_root,
):
    outers, pres, columns = relayed_products(
        inputs,
        query_grad,
        forget_grad,
        forget_pre,
        lower_bound,
        query_row_root,
        forget_row_root,
        query_col_root,
        forget_col_root,
    )
    return tuple(
        finished(
            outers,
            pres,
            columns,
            (query_weight, forget_weight),
            (query_moment, forget_moment),
            (query_rows, forget_rows),
            (query_cols, forget_cols),
        )
    )


def on_device(*args):
    token_count = args[0].shape[0] * lax.axis_size("fs")
    feature_count = args[0].shape[1] * lax.axis_size("tp")
    paired = lax.axis_size("fs") == 8 and lax.axis_size("tp") == 4
    if paired and token_count <= feature_count:
        return gather_plan(*args)
    return reduce_plan(*args)


def solution(mesh):
    in_specs = (
        P("fs", "tp"),
        P("fs", "tp"),
        P("fs", "tp"),
        P("fs", "tp"),
        P("tp"),
        P("fs", "tp"),
        P("fs", "tp"),
        P("fs", "tp"),
        P("fs", "tp"),
        P("fs", None),
        P("fs", None),
        P("tp", None, None),
        P("tp", None, None),
        P("fs", None),
        P("fs", None),
        P("tp", None, None),
        P("tp", None, None),
    )
    out_specs = (
        P("fs", "tp"),
        P("fs", "tp"),
        P("fs", "tp"),
        P("fs", "tp"),
        P("fs", "tp"),
        P("fs", "tp"),
        P("fs", "tp"),
        P("fs", "tp"),
        P("fs", None),
        P("fs", None),
        P("tp", None, None),
        P("tp", None, None),
    )
    return jax.shard_map(
        on_device, mesh=mesh, in_specs=in_specs, out_specs=out_specs, check_vma=False
    )
```

```python
import jax
import jax.numpy as jnp
from jax import lax
from jax.experimental import pallas as pl
from jax.experimental.pallas import tpu as pltpu
from jax.sharding import PartitionSpec as P

D = 2048
HW = 1024
HEAD = 128


stat_decay = 0.9
moment_decay = 0.9
learn_rate = 0.02
highest = lax.Precision.HIGHEST
MESH = pl.DeviceIdType.MESH


def fold_one(carry_state, shard_piece, offset, root_mine, grad_mine):
    left_sum, outer_rows, column_total = carry_state
    row_count, col_width = shard_piece.shape
    left_sum = left_sum + jnp.dot(root_mine, shard_piece, precision=highest)
    outer_piece = lax.dot_general(
        grad_mine, shard_piece, (((1,), (1,)), ((), ())), precision=highest
    )
    outer_rows = lax.dynamic_update_slice_in_dim(outer_rows, outer_piece, offset, 1)
    by_head = shard_piece.reshape(row_count, col_width // HEAD, HEAD)
    column_total = column_total + jnp.einsum("rhi,rhj->hij", by_head, by_head, precision=highest)
    return (left_sum, outer_rows, column_total)


def finish(weight, moment, rows, cols, col_root, left_sum, outer_rows, column_total, square):
    norm_scale = jnp.sqrt(D * HW / (square + 1.0))
    scale_twice = norm_scale * norm_scale
    rows_next = stat_decay * rows + (1.0 - stat_decay) / HW * scale_twice * outer_rows
    cols_next = stat_decay * cols + (1.0 - stat_decay) / D * scale_twice * column_total
    shard_rows, col_width = left_sum.shape
    shaped = left_sum.reshape(shard_rows, col_width // HEAD, HEAD)
    precond = norm_scale * jnp.einsum(
        "rhi,hij->rhj", shaped, col_root.astype(jnp.float32), precision=highest
    ).reshape(shard_rows, col_width)
    moment_next = moment_decay * moment + (1.0 - moment_decay) * precond
    update_step = moment_decay * moment_next + (1.0 - moment_decay) * precond
    master = weight - learn_rate * update_step
    return (master, master.astype(jnp.bfloat16), update_step, moment_next, rows_next, cols_next)


def reduce_plan(
    inputs,
    query_grad,
    forget_grad,
    forget_pre,
    lower_bound,
    query_weight,
    forget_weight,
    query_moment,
    forget_moment,
    query_rows,
    forget_rows,
    query_cols,
    forget_cols,
    query_row_root,
    forget_row_root,
    query_col_root,
    forget_col_root,
):
    sigma_gate = jax.nn.sigmoid(forget_pre.astype(jnp.float32))
    forget_cot = (
        forget_grad.astype(jnp.float32) * (1.0 - lower_bound) * sigma_gate * (1.0 - sigma_gate)
    ).astype(jnp.bfloat16)
    gathered = lax.all_gather(inputs, "tp", axis=1, tiled=True)
    shard_rows, col_width = query_weight.shape
    heads_here = col_width // HEAD
    row_roots = (query_row_root.astype(jnp.float32), forget_row_root.astype(jnp.float32))
    empty = (
        jnp.zeros((shard_rows, col_width), jnp.float32),
        jnp.zeros((shard_rows, D), jnp.float32),
        jnp.zeros((heads_here, HEAD, HEAD), jnp.float32),
    )
    joined = jnp.concatenate([query_grad, forget_cot], axis=1)
    summed = lax.psum_scatter(
        lax.dot_general(
            gathered, joined, (((0,), (0,)), ((), ())), preferred_element_type=jnp.float32
        ),
        "fs",
        scatter_dimension=0,
        tiled=True,
    )
    gradients = (summed[:, :col_width], summed[:, col_width:])
    offset = jnp.int32(0)
    results = (
        fold_one(
            empty,
            lax.all_gather(gradients[0].astype(jnp.bfloat16), "fs", axis=0, tiled=True).astype(
                jnp.float32
            ),
            offset,
            row_roots[0],
            gradients[0],
        ),
        fold_one(
            empty,
            lax.all_gather(gradients[1].astype(jnp.bfloat16), "fs", axis=0, tiled=True).astype(
                jnp.float32
            ),
            offset,
            row_roots[1],
            gradients[1],
        ),
    )
    query_trace = jnp.sum(jnp.diagonal(results[0][2], axis1=1, axis2=2))
    forget_trace = jnp.sum(jnp.diagonal(results[1][2], axis1=1, axis2=2))
    query_outer, forget_outer, query_square, forget_square = (
        lax.psum(results[0][1].astype(jnp.bfloat16), "tp").astype(jnp.float32),
        lax.psum(results[1][1].astype(jnp.bfloat16), "tp").astype(jnp.float32),
        lax.psum(query_trace.astype(jnp.bfloat16), "tp").astype(jnp.float32),
        lax.psum(forget_trace.astype(jnp.bfloat16), "tp").astype(jnp.float32),
    )
    query_out = finish(
        query_weight,
        query_moment,
        query_rows,
        query_cols,
        query_col_root,
        results[0][0],
        query_outer,
        results[0][2],
        query_square,
    )
    forget_out = finish(
        forget_weight,
        forget_moment,
        forget_rows,
        forget_cols,
        forget_col_root,
        results[1][0],
        forget_outer,
        results[1][2],
        forget_square,
    )
    return (
        query_out[0],
        forget_out[0],
        query_out[1],
        forget_out[1],
        query_out[2],
        forget_out[2],
        query_out[3],
        forget_out[3],
        query_out[4],
        forget_out[4],
        query_out[5],
        forget_out[5],
    )


def to_bf16(value):
    return value.astype(jnp.bfloat16)


def wide_dot(left, right, dims):
    return lax.dot_general(left, right, (dims, ((), ())), preferred_element_type=jnp.float32)


LAYERS = "ABCD"
ROUTES = {
    "Ac": ("b", "m", "p", "s"),
    "Bc": ("m", "s"),
    "Cc": ("n", "p", "s"),
    "Dc": ("n", "p", "s"),
    "Ap": ("s", "b"),
    "Cp": ("s",),
    "Dp": ("s",),
    "Ad": ("b",),
}
PROGRAM = (
    "o0", "o2", "o1", "o3", "w2Cc", "w0Bc", "w2Ap", "w1Cc", "w3Bc", "w2Bc", "w1Ap", "w0Cc",
    "w2Cp", "w1Bc", "w1Cp", "w0Ap", "w3Dc", "w0Cp", "w2Bs", "w3As", "w3Ap", "w1Ad", "w0Dc",
    "w0Bp", "w1Cs", "w1Dc", "w3Bs", "w0As", "w3Bp", "w0Cs", "w1Bs", "w3Dp", "w0Ad", "w2Cd",
    "w2As", "w1As", "TA", "w1Bp", "w2Cs", "w3Cc", "w0Bs", "w0Cd", "w2Dc", "w0Bd", "w2Ad", "w1Dp",
    "w1Cd", "TC", "w3Ad", "w0Ds", "w0Dp", "w3Cp", "w1Bd", "TB", "w3Ds", "w2Bp", "w2Bd",
    ("G2ABC", ("w2Dp",), ("w3Dd",), ("w0Dd",)), "w2Ds", "w1Dd", "w3Bd", "w3Cs", "w3Cd",
    ("G3ABC", ("w1Ds",), ("w2Dd",)), "TD", ("G2D",), "S01", "L", "Q", ("G3D",), "S23", "P",
)


def relay_kernel(
    x_hbm, q_hbm, g_hbm, pre_hbm, bound_ref, rq_hbm, rf_hbm, cq_hbm, cf_hbm,
    wq_hbm, wf_hbm, mq_hbm, mf_hbm, hq_hbm, hf_hbm, vq_hbm, vf_hbm,
    s_ref, pre_ref, k_ref, weight_ref, moment_ref, rows_ref, cols_ref,
    xs, gs, go, xt, acc, grad, sacc, norms, roots, col_roots, raw, turn,
    own_sem, send_sem, x_sem, g_sem, o_sem, swap_sem,
):
    shards, parts, block, span = xs.shape
    width = go.shape[2]
    features = xt.shape[0]
    chunk = s_ref.shape[1]
    heads = width // HEAD
    f32 = jnp.float32
    fs = lax.axis_index("fs")
    tp = lax.axis_index("tp")
    z, px = lax.div(fs, 2), lax.rem(fs, 2)
    py, pc = lax.div(tp, 2), lax.rem(tp, 2)
    pair = z + 1 - 2 * lax.rem(z, 2)
    low = z < 2
    near = jnp.where(low, 2, 1)
    layer = {"A": z, "B": pair, "C": near, "D": jnp.where(low, 3, 0)}
    middle = jnp.logical_and(z > 0, z < 3)
    flips = {"c": (0, 0), "p": (1 - pc, pc), "s": (pc, 1 - pc), "d": (1, 1)}

    def column(who):
        flip_x, flip_y = flips[who]
        return px + flip_x - 2 * px * flip_x, py + flip_y - 2 * py * flip_y

    def device(link):
        if link in ("b", "n"):
            return (2 * pair + px, tp)
        if link == "m":
            return (2 * near + px, tp)
        if link == "core":
            return (fs, tp + 1 - 2 * pc)
        x, y = column(link)
        return (2 * z + x, 2 * y + pc)

    beside = {link: device(link) for link in ("b", "n", "m", "p", "s", "core")}
    conds = {"n": middle, "m": middle}
    aside = {"c": None, "p": pc == 0, "s": pc == 1}

    def guarded(cond, action):
        if cond is None:
            action()
        else:
            pl.when(cond)(action)

    barrier = pltpu.get_barrier_semaphore()

    def greet(name):
        pl.semaphore_signal(barrier, inc=1, device_id=beside[name], device_id_type=MESH)

    for name in ("b", "p", "s", "core"):
        greet(name)
    guarded(middle, lambda: greet("m"))
    loads = [
        pltpu.make_async_copy(source, target, own_sem.at[number])
        for number, (source, target) in enumerate(
            (
                (x_hbm, xs.at[fs, tp]),
                (q_hbm, raw.at[0]),
                (g_hbm, raw.at[1]),
                (pre_hbm, raw.at[2]),
                (rq_hbm, roots.at[0]),
                (rf_hbm, roots.at[1]),
                (cq_hbm, col_roots.at[0]),
                (cf_hbm, col_roots.at[1]),
                (wq_hbm, weight_ref.at[0]),
                (wf_hbm, weight_ref.at[1]),
                (mq_hbm, moment_ref.at[0]),
                (mf_hbm, moment_ref.at[1]),
                (hq_hbm, rows_ref.at[0]),
                (hf_hbm, rows_ref.at[1]),
                (vq_hbm, cols_ref.at[0]),
                (vf_hbm, cols_ref.at[1]),
            )
        )
    ]
    for load in loads[:4]:
        load.start()
    for load in loads[1:4]:
        load.wait()
    sigma_gate = jax.nn.sigmoid(raw[2].astype(f32))
    cot = to_bf16(
        raw[1].astype(f32) * (1.0 - bound_ref[...]) * sigma_gate * (1.0 - sigma_gate)
    )

    @pl.when(pc == 0)
    def _():
        gs[fs, py, 0] = raw[0]
        go[fs] = cot

    @pl.when(pc == 1)
    def _():
        gs[fs, py, 1] = cot
        go[fs] = raw[0]

    loads[0].wait()
    pl.semaphore_wait(barrier, 4 + jnp.where(middle, 1, 0))

    for load in loads[4:]:
        load.start()
    half_rows = block // 2
    pending = []
    dones = []

    def halves(phase):
        return 1 - pc if phase == 2 else pc

    def piece(phase, name):
        x, y = column(name[1])
        shard = 2 * layer[name[0]] + x
        if phase < 2:
            rows = pl.ds(phase * half_rows, half_rows)
            part = 2 * y + pc
            return xs.at[shard, part, rows], x_sem.at[phase, shard, part]
        return gs.at[shard, y, halves(phase)], g_sem.at[phase - 2, shard, y]

    def start(recipe, link, cond=None):
        number = len(pending)

        def build():
            src, dst, sem = recipe()
            return pltpu.make_async_remote_copy(
                src_ref=src, dst_ref=dst, send_sem=send_sem.at[number], recv_sem=sem,
                device_id=beside[link], device_id_type=MESH,
            )

        guarded(cond, lambda: build().start())
        pending.append((cond, build))

    def landed(ref, sem):
        pltpu.make_async_remote_copy(
            src_ref=ref, dst_ref=ref, send_sem=send_sem.at[0], recv_sem=sem,
            device_id=beside["core"], device_id_type=MESH,
        ).wait_recv()

    def forward(phase, name):
        def same():
            here, sem = piece(phase, name)
            return here, here, sem

        def beyond():
            here, _ = piece(phase, name)
            shard = 2 * layer[name[0]] + column(name[1])[0]
            return here, go.at[shard], o_sem.at[shard]

        for link in ROUTES.get(name, ()):
            start(same, link, conds.get(link))
        if phase < 2:
            start(same, "core")
        if phase == 2 and name != "Ac" and name[1] != "d":
            start(beyond, "core", aside[name[1]])

    start(lambda: (go.at[fs], gs.at[fs, py, pc], g_sem.at[0, fs, py]), "core")

    def from_core(label):
        for phase in range(2):
            for x in range(2):
                for y in range(2):
                    shard, part = 2 * layer[label] + x, 2 * y + 1 - pc
                    rows = pl.ds(phase * half_rows, half_rows)
                    landed(xs.at[shard, part, rows], x_sem.at[phase, shard, part])

    def transpose(label):
        at = LAYERS.index(label)

        @pl.loop(0, 2)
        def _(x):
            lanes = pl.ds(pl.multiple_of((2 * at + x) * block, block), block)
            for part in range(parts):
                turned = xs[2 * layer[label] + x, part].T
                xt[part * span : (part + 1) * span, lanes] = turned

    squares = []
    tile = features // 4

    def own_block(phase, far, label):
        y = 1 - py if far else py
        both = pl.ds(2 * layer[label], 2)
        return gs[both, y, halves(phase)].reshape(2 * block, width)

    def other_block(label):
        return go[pl.ds(2 * layer[label], 2)].reshape(2 * block, width)

    def gradients(phase, labels, events):
        first, final = labels[0] == LAYERS[0], labels[-1] == LAYERS[-1]
        start_token = LAYERS.index(labels[0]) * 2 * block
        tokens = slice(start_token, start_token + len(labels) * 2 * block)
        if phase == 2:
            for label in labels:
                for x in range(2):
                    shard = 2 * layer[label] + x
                    guarded(
                        px != x if label == "A" else None,
                        lambda shard=shard: landed(go.at[shard], o_sem.at[shard]),
                    )

        def body(step, total):
            rows = pl.ds(pl.multiple_of(step * tile, tile), tile)
            for far in range(3 if phase == 2 else 2):
                at = 4 if far == 2 else 2 * (phase - 2) + far
                right = jnp.concatenate(
                    [other_block(k) if far == 2 else own_block(phase, far, k) for k in labels], axis=0
                )
                value = wide_dot(xt[rows, tokens], right, ((1,), (0,)))
                if not first:
                    value = value + acc[at, rows, :]
                if final:
                    grad[rows, at * width : (at + 1) * width] = to_bf16(value)
                    if far < 2:
                        squared = (value * value).reshape(tile // 8, 8, width)
                        total = total + jnp.sum(squared, axis=0)
                else:
                    acc[at, rows, :] = value
            for number, names in enumerate(events):
                if names:

                    @pl.when(step == number)
                    def _(names=names):
                        for name in names:
                            travel(name)

            return total

        total = lax.fori_loop(0, features // tile, body, jnp.zeros((8, width), f32))
        if final:
            squares.append(total)

    mine = pl.ds(pl.multiple_of(fs * chunk, chunk), chunk)
    hidden = parts * width
    size = float(features * hidden)

    def outer_step(lanes, first, final):
        wide = 2 * chunk
        if final:
            square = jnp.sum(squares[0], axis=(0, 1), keepdims=True)
            for more in squares[1:]:
                square = square + jnp.sum(more, axis=(0, 1), keepdims=True)
            norms[0] = jnp.broadcast_to(square, norms.shape[1:])
            scale = (1.0 - stat_decay) / hidden * (size / (square + 1.0))
            swap_norm = pltpu.make_async_remote_copy(
                src_ref=norms.at[0], dst_ref=norms.at[1],
                send_sem=swap_sem.at[0], recv_sem=swap_sem.at[1],
                device_id=beside["core"], device_id_type=MESH,
            )
        if not final:

            @pl.loop(0, features // wide)
            def _(step):
                rows = pl.ds(pl.multiple_of(step * wide, wide), wide)
                product = wide_dot(grad[mine, lanes], grad[rows, lanes], ((1,), (1,)))
                if not first:
                    product = product + sacc[:, rows]
                sacc[:, rows] = product

            return
        for step in range(features // wide):
            rows = slice(step * wide, (step + 1) * wide)
            product = wide_dot(grad[mine, lanes], grad[rows, lanes], ((1,), (1,)))
            s_ref[pc, :, rows] = to_bf16((product + sacc[:, rows]) * scale)
            if step == 0:
                swap_norm.start()
                dones.append(swap_norm)
            else:
                send_outer(step - 1)
        send_outer(features // wide - 1)

    def outer_copy(which, step):
        rows = pl.ds(step * 2 * chunk, 2 * chunk)
        return pltpu.make_async_remote_copy(
            src_ref=s_ref.at[which, :, rows], dst_ref=s_ref.at[which, :, rows],
            send_sem=swap_sem.at[2 + step], recv_sem=swap_sem.at[6 + step],
            device_id=beside["core"], device_id_type=MESH,
        )

    def send_outer(step):
        outer_copy(pc, step).start()
        dones.append(step)

    def products(which, lanes):
        for step in range(features // chunk):
            rows = slice(step * chunk, (step + 1) * chunk)
            turn[:, rows] = grad[rows, lanes].T
        left = wide_dot(roots[which], grad[:, lanes], ((1,), (0,)))
        gram = wide_dot(turn[...], grad[:, lanes], ((1,), (0,)))
        for head in range(heads):
            at = slice(head * HEAD, (head + 1) * HEAD)
            k_ref[which, head] = gram[at, at]
            pre_ref[which, :, at] = wide_dot(
                to_bf16(left[:, at]), col_roots[which, head], ((1,), (0,))
            )

    def travel(op):
        phase = int(op[1])
        if op[0] == "w" or phase == 2:
            landed(*piece(phase, op[2:] or "Ac"))
        forward(phase, op[2:] or "Ac")

    for op in PROGRAM:
        kind, rest = op[0], op[1:]
        if isinstance(op, tuple):
            gradients(int(op[0][1]), op[0][2:], op[1:])
        elif kind in "ow":
            travel(op)
        elif kind == "T":
            from_core(rest)
            transpose(rest)
        elif kind == "S":
            first, last = int(rest[0]), int(rest[1])
            outer_step(slice(first * width, (last + 1) * width), first == 0, last == 3)
        elif kind == "L":
            for load in loads[4:8]:
                load.wait()
        elif kind == "P":
            products(pc, slice(2 * width, 3 * width))
        elif kind == "Q":
            products(1 - pc, slice(4 * width, 5 * width))

    dones[0].wait()
    mine_sum, their_sum = norms[0, 0:1, 0:1], norms[1, 0:1, 0:1]
    sums = (
        jnp.where(pc == 0, mine_sum, their_sum),
        jnp.where(pc == 0, their_sum, mine_sum),
    )
    for which in range(2):
        scale_twice = size / (sums[which] + 1.0)
        pre_ref[which] = pre_ref[which] * jnp.sqrt(scale_twice)
        for head in range(heads):
            k_ref[which, head] = k_ref[which, head] * (
                (1.0 - stat_decay) / features * scale_twice
            )
    for step in dones[1:]:
        outer_copy(pc, step).wait_send()
        outer_copy(1 - pc, step).wait_recv()
    for load in loads[8:]:
        load.wait()
    for cond, build in pending:
        guarded(cond, lambda build=build: build().wait_send())


def in_hbm(*arrays):
    return [pltpu.with_memory_space_constraint(array, pltpu.HBM) for array in arrays]


def relayed_products(x, query_grad, forget_grad, forget_pre, lower_bound, *held):
    shards, parts = lax.axis_size("fs"), lax.axis_size("tp")
    block, span = x.shape
    width = query_grad.shape[1]
    chunk, features = held[0].shape
    bf16, f32 = jnp.bfloat16, jnp.float32
    heads = held[2].shape
    vmem = pl.BlockSpec(memory_space=pltpu.VMEM)
    hbm = pl.BlockSpec(memory_space=pltpu.HBM)
    return pl.pallas_call(
        relay_kernel,
        out_shape=[
            pltpu.VMEM((2, chunk, features), bf16),
            pltpu.VMEM((2, chunk, width), f32),
            pltpu.VMEM((2,) + heads, f32),
            pltpu.VMEM((2, chunk, width), f32),
            pltpu.VMEM((2, chunk, width), f32),
            pltpu.VMEM((2, chunk, features), f32),
            pltpu.VMEM((2,) + heads, f32),
        ],
        in_specs=[hbm] * 4 + [vmem] + [hbm] * 12,
        out_specs=[vmem] * 7,
        scratch_shapes=[
            pltpu.VMEM((shards, parts, block, span), bf16),
            pltpu.VMEM((shards, 2, 2, block, width), bf16),
            pltpu.VMEM((shards, block, width), bf16),
            pltpu.VMEM((features, shards * block), bf16),
            pltpu.VMEM((parts + 1, features, width), f32),
            pltpu.VMEM((features, (parts + 1) * width), bf16),
            pltpu.VMEM((chunk, features), f32),
            pltpu.VMEM((2, 8, 128), f32),
            pltpu.VMEM((2, chunk, features), bf16),
            pltpu.VMEM((2,) + heads, bf16),
            pltpu.VMEM((3, block, width), bf16),
            pltpu.VMEM((width, features), bf16),
            pltpu.SemaphoreType.DMA((16,)),
            pltpu.SemaphoreType.DMA((128,)),
            pltpu.SemaphoreType.DMA((2, shards, parts)),
            pltpu.SemaphoreType.DMA((2, shards, 2)),
            pltpu.SemaphoreType.DMA((shards,)),
            pltpu.SemaphoreType.DMA((10,)),
        ],
        compiler_params=pltpu.CompilerParams(
            collective_id=0, has_side_effects=True, vmem_limit_bytes=48 * 1024 * 1024
        ),
    )(
        *in_hbm(x, query_grad, forget_grad, forget_pre), lower_bound.reshape(1, -1), *in_hbm(*held)
    )


def finish_kernel(outer_ref, pre_ref, column_ref, weight_ref, moment_ref, rows_ref, cols_ref, *outs):
    step = pl.program_id(0)
    tile, head_tile = outs[0].shape[0], outs[10].shape[1]
    at = pl.ds(pl.multiple_of(step * tile, tile), tile)
    head_at = pl.ds(pl.multiple_of(step * head_tile, head_tile), head_tile)
    for which in range(2):
        master_out, copy_out, step_out, moment_out, rows_out, cols_out = outs[which::2]
        precond = pre_ref[which, at, :]
        moment_next = moment_decay * moment_ref[which, at, :] + (1.0 - moment_decay) * precond
        update_step = moment_decay * moment_next + (1.0 - moment_decay) * precond
        master = weight_ref[which, at, :] - learn_rate * update_step
        master_out[...] = master
        copy_out[...] = to_bf16(master)
        step_out[...] = update_step
        moment_out[...] = moment_next
        rows_out[...] = stat_decay * rows_ref[which, at, :] + outer_ref[which, at, :].astype(
            jnp.float32
        )
        cols_out[...] = (
            stat_decay * cols_ref[which, :, head_at, :] + column_ref[which, :, head_at, :]
        )


def finished(held):
    f32, bf16 = jnp.float32, jnp.bfloat16
    _, chunk, features = held[0].shape
    width = held[1].shape[2]
    heads = held[2].shape[1:]
    steps = 4
    tile = chunk // steps
    narrow = pl.BlockSpec((tile, width), lambda i: (i, 0))
    wide = pl.BlockSpec((tile, features), lambda i: (i, 0))
    head = pl.BlockSpec((heads[0], heads[1] // steps, heads[2]), lambda i: (0, i, 0))
    flat = lambda kind: [jax.ShapeDtypeStruct((chunk, width), kind)] * 2
    return pl.pallas_call(
        finish_kernel,
        grid=(steps,),
        out_shape=flat(f32)
        + flat(bf16)
        + flat(f32)
        + flat(f32)
        + [jax.ShapeDtypeStruct((chunk, features), f32)] * 2
        + [jax.ShapeDtypeStruct(heads, f32)] * 2,
        in_specs=[pl.BlockSpec(memory_space=pltpu.VMEM)] * 7,
        out_specs=[narrow] * 8 + [wide] * 2 + [head] * 2,
        compiler_params=pltpu.CompilerParams(vmem_limit_bytes=24 * 1024 * 1024),
    )(*[pltpu.with_memory_space_constraint(array, pltpu.VMEM) for array in held])


def gather_plan(
    inputs,
    query_grad,
    forget_grad,
    forget_pre,
    lower_bound,
    query_weight,
    forget_weight,
    query_moment,
    forget_moment,
    query_rows,
    forget_rows,
    query_cols,
    forget_cols,
    query_row_root,
    forget_row_root,
    query_col_root,
    forget_col_root,
):
    held = relayed_products(
        inputs,
        query_grad,
        forget_grad,
        forget_pre,
        lower_bound,
        query_row_root,
        forget_row_root,
        query_col_root,
        forget_col_root,
        query_weight,
        forget_weight,
        query_moment,
        forget_moment,
        query_rows,
        forget_rows,
        query_cols,
        forget_cols,
    )
    return tuple(finished(held))


def on_device(*args):
    token_count = args[0].shape[0] * lax.axis_size("fs")
    feature_count = args[0].shape[1] * lax.axis_size("tp")
    paired = lax.axis_size("fs") == 8 and lax.axis_size("tp") == 4
    if paired and token_count <= feature_count:
        return gather_plan(*args)
    return reduce_plan(*args)


def solution(mesh):
    in_specs = (
        P("fs", "tp"),
        P("fs", "tp"),
        P("fs", "tp"),
        P("fs", "tp"),
        P("tp"),
        P("fs", "tp"),
        P("fs", "tp"),
        P("fs", "tp"),
        P("fs", "tp"),
        P("fs", None),
        P("fs", None),
        P("tp", None, None),
        P("tp", None, None),
        P("fs", None),
        P("fs", None),
        P("tp", None, None),
        P("tp", None, None),
    )
    out_specs = (
        P("fs", "tp"),
        P("fs", "tp"),
        P("fs", "tp"),
        P("fs", "tp"),
        P("fs", "tp"),
        P("fs", "tp"),
        P("fs", "tp"),
        P("fs", "tp"),
        P("fs", None),
        P("fs", None),
        P("tp", None, None),
        P("tp", None, None),
    )
    return jax.shard_map(
        on_device, mesh=mesh, in_specs=in_specs, out_specs=out_specs, check_vma=False
    )
```

```python
import jax
import jax.numpy as jnp
from jax import lax
from jax.experimental import pallas as pl
from jax.experimental.pallas import tpu as pltpu
from jax.sharding import PartitionSpec as P

D = 2048
HW = 1024
HEAD = 128


stat_decay = 0.9
moment_decay = 0.9
learn_rate = 0.02
highest = lax.Precision.HIGHEST
MESH = pl.DeviceIdType.MESH


def fold_one(carry_state, shard_piece, offset, root_mine, grad_mine):
    left_sum, outer_rows, column_total = carry_state
    row_count, col_width = shard_piece.shape
    left_sum = left_sum + jnp.dot(root_mine, shard_piece, precision=highest)
    outer_piece = lax.dot_general(
        grad_mine, shard_piece, (((1,), (1,)), ((), ())), precision=highest
    )
    outer_rows = lax.dynamic_update_slice_in_dim(outer_rows, outer_piece, offset, 1)
    by_head = shard_piece.reshape(row_count, col_width // HEAD, HEAD)
    column_total = column_total + jnp.einsum("rhi,rhj->hij", by_head, by_head, precision=highest)
    return (left_sum, outer_rows, column_total)


def finish(weight, moment, rows, cols, col_root, left_sum, outer_rows, column_total, square):
    norm_scale = jnp.sqrt(D * HW / (square + 1.0))
    scale_twice = norm_scale * norm_scale
    rows_next = stat_decay * rows + (1.0 - stat_decay) / HW * scale_twice * outer_rows
    cols_next = stat_decay * cols + (1.0 - stat_decay) / D * scale_twice * column_total
    shard_rows, col_width = left_sum.shape
    shaped = left_sum.reshape(shard_rows, col_width // HEAD, HEAD)
    precond = norm_scale * jnp.einsum(
        "rhi,hij->rhj", shaped, col_root.astype(jnp.float32), precision=highest
    ).reshape(shard_rows, col_width)
    moment_next = moment_decay * moment + (1.0 - moment_decay) * precond
    update_step = moment_decay * moment_next + (1.0 - moment_decay) * precond
    master = weight - learn_rate * update_step
    return (master, master.astype(jnp.bfloat16), update_step, moment_next, rows_next, cols_next)


def reduce_plan(
    inputs,
    query_grad,
    forget_grad,
    forget_pre,
    lower_bound,
    query_weight,
    forget_weight,
    query_moment,
    forget_moment,
    query_rows,
    forget_rows,
    query_cols,
    forget_cols,
    query_row_root,
    forget_row_root,
    query_col_root,
    forget_col_root,
):
    sigma_gate = jax.nn.sigmoid(forget_pre.astype(jnp.float32))
    forget_cot = (
        forget_grad.astype(jnp.float32) * (1.0 - lower_bound) * sigma_gate * (1.0 - sigma_gate)
    ).astype(jnp.bfloat16)
    gathered = lax.all_gather(inputs, "tp", axis=1, tiled=True)
    shard_rows, col_width = query_weight.shape
    heads_here = col_width // HEAD
    row_roots = (query_row_root.astype(jnp.float32), forget_row_root.astype(jnp.float32))
    empty = (
        jnp.zeros((shard_rows, col_width), jnp.float32),
        jnp.zeros((shard_rows, D), jnp.float32),
        jnp.zeros((heads_here, HEAD, HEAD), jnp.float32),
    )
    joined = jnp.concatenate([query_grad, forget_cot], axis=1)
    summed = lax.psum_scatter(
        lax.dot_general(
            gathered, joined, (((0,), (0,)), ((), ())), preferred_element_type=jnp.float32
        ),
        "fs",
        scatter_dimension=0,
        tiled=True,
    )
    gradients = (summed[:, :col_width], summed[:, col_width:])
    offset = jnp.int32(0)
    results = (
        fold_one(
            empty,
            lax.all_gather(gradients[0].astype(jnp.bfloat16), "fs", axis=0, tiled=True).astype(
                jnp.float32
            ),
            offset,
            row_roots[0],
            gradients[0],
        ),
        fold_one(
            empty,
            lax.all_gather(gradients[1].astype(jnp.bfloat16), "fs", axis=0, tiled=True).astype(
                jnp.float32
            ),
            offset,
            row_roots[1],
            gradients[1],
        ),
    )
    query_trace = jnp.sum(jnp.diagonal(results[0][2], axis1=1, axis2=2))
    forget_trace = jnp.sum(jnp.diagonal(results[1][2], axis1=1, axis2=2))
    query_outer, forget_outer, query_square, forget_square = (
        lax.psum(results[0][1].astype(jnp.bfloat16), "tp").astype(jnp.float32),
        lax.psum(results[1][1].astype(jnp.bfloat16), "tp").astype(jnp.float32),
        lax.psum(query_trace.astype(jnp.bfloat16), "tp").astype(jnp.float32),
        lax.psum(forget_trace.astype(jnp.bfloat16), "tp").astype(jnp.float32),
    )
    query_out = finish(
        query_weight,
        query_moment,
        query_rows,
        query_cols,
        query_col_root,
        results[0][0],
        query_outer,
        results[0][2],
        query_square,
    )
    forget_out = finish(
        forget_weight,
        forget_moment,
        forget_rows,
        forget_cols,
        forget_col_root,
        results[1][0],
        forget_outer,
        results[1][2],
        forget_square,
    )
    return (
        query_out[0],
        forget_out[0],
        query_out[1],
        forget_out[1],
        query_out[2],
        forget_out[2],
        query_out[3],
        forget_out[3],
        query_out[4],
        forget_out[4],
        query_out[5],
        forget_out[5],
    )


def to_bf16(value):
    return value.astype(jnp.bfloat16)


def wide_dot(left, right, dims):
    return lax.dot_general(left, right, (dims, ((), ())), preferred_element_type=jnp.float32)


LAYERS = "ABCD"
ROUTES = {
    "Ac": ("b", "m", "p", "s"),
    "Bc": ("m", "s"),
    "Cc": ("n", "p", "s"),
    "Dc": ("n", "p", "s"),
    "Ap": ("s", "b"),
    "Cp": ("s",),
    "Dp": ("s",),
    "Ad": ("b",),
}
PROGRAM = (
    "o0", "o1", "C", "o3", "o2", "w0Bc", "w0Cc", "w1Bc", "w0Ap", "w2Bc", "w0As", "w3Cc", "w1As",
    "w1Cc", "w1Ap", "w0Dc", "w0Cp", "w0Ad", "w2Ap", "w1Cp", "w1Bs", "w1Cs", "w3Bc", "w2Cc",
    "w0Cs", "w1Dc", "w2Dc", "w1Cd", "w3Cs", "w2Cp", "w0Bs", "w2Bs", "w0Cd", "w3Cp", "w0Ds",
    "w2Bp", "w1Ad", "TC", "TA", "w1Bp", "w3Dc", "w2Ad", "w1Dp", "w0Bd", "w1Ds", "w3Bs", "w0Dp",
    "w0Bp", "w2Cs", "w1Bd", "w3As", "w2As", "TB", "w3Cd", "w3Ap", "w2Dp", "w2Cd", "w2Ds", "w2Bd",
    ("G2ABC", ("w3Ds",), ("w1Dd",), ("w0Dd", "w3Dp", "w3Ad", "w3Bp",)), "TD", "w2Dd", ("G2D",),
    "S01", "w3Dd", "L", "Q", "w3Bd", ("G3ABC",), ("G3D",), "S23", "P",
)


def relay_kernel(
    x_hbm, q_hbm, g_hbm, pre_hbm, bound_hbm, rq_hbm, rf_hbm, cq_hbm, cf_hbm,
    wq_hbm, wf_hbm, mq_hbm, mf_hbm, hq_hbm, hf_hbm, vq_hbm, vf_hbm,
    s_ref, pre_ref, k_ref, weight_ref, moment_ref, rows_ref, cols_ref,
    xs, gs, go, xt, acc, grad, sacc, norms, roots, col_roots, raw, bound, turn,
    own_sem, send_sem, x_sem, g_sem, o_sem, swap_sem,
):
    shards, parts, block, span = xs.shape
    width = go.shape[2]
    features = xt.shape[0]
    chunk = s_ref.shape[1]
    heads = width // HEAD
    f32 = jnp.float32
    fs = lax.axis_index("fs")
    tp = lax.axis_index("tp")
    z, px = lax.div(fs, 2), lax.rem(fs, 2)
    py, pc = lax.div(tp, 2), lax.rem(tp, 2)
    pair = z + 1 - 2 * lax.rem(z, 2)
    low = z < 2
    near = jnp.where(low, 2, 1)
    layer = {"A": z, "B": pair, "C": near, "D": jnp.where(low, 3, 0)}
    middle = jnp.logical_and(z > 0, z < 3)
    flips = {"c": (0, 0), "p": (1 - pc, pc), "s": (pc, 1 - pc), "d": (1, 1)}

    def column(who):
        flip_x, flip_y = flips[who]
        return px + flip_x - 2 * px * flip_x, py + flip_y - 2 * py * flip_y

    def device(link):
        if link in ("b", "n"):
            return (2 * pair + px, tp)
        if link == "m":
            return (2 * near + px, tp)
        if link == "core":
            return (fs, tp + 1 - 2 * pc)
        x, y = column(link)
        return (2 * z + x, 2 * y + pc)

    beside = {link: device(link) for link in ("b", "n", "m", "p", "s", "core")}
    conds = {"n": middle, "m": middle}
    aside = {"c": None, "p": pc == 0, "s": pc == 1}

    def guarded(cond, action):
        if cond is None:
            action()
        else:
            pl.when(cond)(action)

    barrier = pltpu.get_barrier_semaphore()

    def greet(name):
        pl.semaphore_signal(barrier, inc=1, device_id=beside[name], device_id_type=MESH)

    for name in ("b", "p", "s", "core"):
        greet(name)
    guarded(middle, lambda: greet("m"))
    loads = [
        pltpu.make_async_copy(source, target, own_sem.at[number])
        for number, (source, target) in enumerate(
            (
                (x_hbm, xs.at[fs, tp]),
                (q_hbm, raw.at[0]),
                (g_hbm, raw.at[1]),
                (pre_hbm, raw.at[2]),
                (bound_hbm, bound),
                (rq_hbm, roots.at[0]),
                (rf_hbm, roots.at[1]),
                (cq_hbm, col_roots.at[0]),
                (cf_hbm, col_roots.at[1]),
                (wq_hbm, weight_ref.at[0]),
                (wf_hbm, weight_ref.at[1]),
                (mq_hbm, moment_ref.at[0]),
                (mf_hbm, moment_ref.at[1]),
                (hq_hbm, rows_ref.at[0]),
                (hf_hbm, rows_ref.at[1]),
                (vq_hbm, cols_ref.at[0]),
                (vf_hbm, cols_ref.at[1]),
            )
        )
    ]
    for load in loads[:5]:
        load.start()
    loads[0].wait()
    pl.semaphore_wait(barrier, 4 + jnp.where(middle, 1, 0))

    def cotangents():
        for load in loads[1:5]:
            load.wait()
        sigma_gate = jax.nn.sigmoid(raw[2].astype(f32))
        cot = to_bf16(
            raw[1].astype(f32) * (1.0 - bound[...]) * sigma_gate * (1.0 - sigma_gate)
        )

        @pl.when(pc == 0)
        def _():
            gs[fs, py, 0] = raw[0]
            go[fs] = cot

        @pl.when(pc == 1)
        def _():
            gs[fs, py, 1] = cot
            go[fs] = raw[0]

        for load in loads[5:]:
            load.start()
        start(lambda: (go.at[fs], gs.at[fs, py, pc], g_sem.at[0, fs, py]), "core")

    half_rows = block // 2
    pending = []
    dones = []

    def halves(phase):
        return 1 - pc if phase == 2 else pc

    def piece(phase, name):
        x, y = column(name[1])
        shard = 2 * layer[name[0]] + x
        if phase < 2:
            rows = pl.ds(phase * half_rows, half_rows)
            part = 2 * y + pc
            return xs.at[shard, part, rows], x_sem.at[phase, shard, part]
        return gs.at[shard, y, halves(phase)], g_sem.at[phase - 2, shard, y]

    def start(recipe, link, cond=None):
        number = len(pending)

        def build():
            src, dst, sem = recipe()
            return pltpu.make_async_remote_copy(
                src_ref=src, dst_ref=dst, send_sem=send_sem.at[number], recv_sem=sem,
                device_id=beside[link], device_id_type=MESH,
            )

        guarded(cond, lambda: build().start())
        pending.append((cond, build))

    def landed(ref, sem):
        pltpu.make_async_remote_copy(
            src_ref=ref, dst_ref=ref, send_sem=send_sem.at[0], recv_sem=sem,
            device_id=beside["core"], device_id_type=MESH,
        ).wait_recv()

    def forward(phase, name):
        def same():
            here, sem = piece(phase, name)
            return here, here, sem

        def beyond():
            here, _ = piece(phase, name)
            shard = 2 * layer[name[0]] + column(name[1])[0]
            return here, go.at[shard], o_sem.at[shard]

        for link in ROUTES.get(name, ()):
            start(same, link, conds.get(link))
        if phase < 2:
            start(same, "core")
        if phase == 2 and name != "Ac" and name[1] != "d":
            start(beyond, "core", aside[name[1]])

    def from_core(label):
        for phase in range(2):
            for x in range(2):
                for y in range(2):
                    shard, part = 2 * layer[label] + x, 2 * y + 1 - pc
                    rows = pl.ds(phase * half_rows, half_rows)
                    landed(xs.at[shard, part, rows], x_sem.at[phase, shard, part])

    def transpose(label):
        at = LAYERS.index(label)

        @pl.loop(0, 2)
        def _(x):
            lanes = pl.ds(pl.multiple_of((2 * at + x) * block, block), block)
            for part in range(parts):
                turned = xs[2 * layer[label] + x, part].T
                xt[part * span : (part + 1) * span, lanes] = turned

    squares = []
    tile = features // 4

    def own_block(phase, far, label):
        y = 1 - py if far else py
        both = pl.ds(2 * layer[label], 2)
        return gs[both, y, halves(phase)].reshape(2 * block, width)

    def other_block(label):
        return go[pl.ds(2 * layer[label], 2)].reshape(2 * block, width)

    def gradients(phase, labels, events):
        first, final = labels[0] == LAYERS[0], labels[-1] == LAYERS[-1]
        start_token = LAYERS.index(labels[0]) * 2 * block
        tokens = slice(start_token, start_token + len(labels) * 2 * block)
        if phase == 2:
            for label in labels:
                for x in range(2):
                    shard = 2 * layer[label] + x
                    guarded(
                        px != x if label == "A" else None,
                        lambda shard=shard: landed(go.at[shard], o_sem.at[shard]),
                    )

        def body(step, total):
            rows = pl.ds(pl.multiple_of(step * tile, tile), tile)
            for far in range(3 if phase == 2 else 2):
                at = 4 if far == 2 else 2 * (phase - 2) + far
                right = jnp.concatenate(
                    [other_block(k) if far == 2 else own_block(phase, far, k) for k in labels], axis=0
                )
                value = wide_dot(xt[rows, tokens], right, ((1,), (0,)))
                if not first:
                    value = value + acc[at, rows, :]
                if final:
                    grad[rows, at * width : (at + 1) * width] = to_bf16(value)
                    if far < 2:
                        squared = (value * value).reshape(tile // 8, 8, width)
                        total = total + jnp.sum(squared, axis=0)
                else:
                    acc[at, rows, :] = value
            for number, names in enumerate(events):
                if names:

                    @pl.when(step == number)
                    def _(names=names):
                        for name in names:
                            travel(name)

            return total

        total = lax.fori_loop(0, features // tile, body, jnp.zeros((8, width), f32))
        if final:
            squares.append(total)

    mine = pl.ds(pl.multiple_of(fs * chunk, chunk), chunk)
    hidden = parts * width
    size = float(features * hidden)

    def outer_step(lanes, first, final):
        wide = 2 * chunk
        if final:
            square = jnp.sum(squares[0], axis=(0, 1), keepdims=True)
            for more in squares[1:]:
                square = square + jnp.sum(more, axis=(0, 1), keepdims=True)
            norms[0] = jnp.broadcast_to(square, norms.shape[1:])
            scale = (1.0 - stat_decay) / hidden * (size / (square + 1.0))
            swap_norm = pltpu.make_async_remote_copy(
                src_ref=norms.at[0], dst_ref=norms.at[1],
                send_sem=swap_sem.at[0], recv_sem=swap_sem.at[1],
                device_id=beside["core"], device_id_type=MESH,
            )
        if not final:

            @pl.loop(0, features // wide)
            def _(step):
                rows = pl.ds(pl.multiple_of(step * wide, wide), wide)
                product = wide_dot(grad[mine, lanes], grad[rows, lanes], ((1,), (1,)))
                if not first:
                    product = product + sacc[:, rows]
                sacc[:, rows] = product

            return
        for step in range(features // wide):
            rows = slice(step * wide, (step + 1) * wide)
            product = wide_dot(grad[mine, lanes], grad[rows, lanes], ((1,), (1,)))
            s_ref[pc, :, rows] = to_bf16((product + sacc[:, rows]) * scale)
            if step == 0:
                swap_norm.start()
                dones.append(swap_norm)
            else:
                send_outer(step - 1)
        for load in loads[9:]:
            load.wait()
        send_outer(features // wide - 1)

    def outer_copy(which, step):
        rows = pl.ds(step * 2 * chunk, 2 * chunk)
        return pltpu.make_async_remote_copy(
            src_ref=s_ref.at[which, :, rows], dst_ref=s_ref.at[which, :, rows],
            send_sem=swap_sem.at[2 + step], recv_sem=swap_sem.at[6 + step],
            device_id=beside["core"], device_id_type=MESH,
        )

    def send_outer(step):
        outer_copy(pc, step).start()
        dones.append(step)

    def products(which, lanes):
        for step in range(features // chunk):
            rows = slice(step * chunk, (step + 1) * chunk)
            turn[:, rows] = grad[rows, lanes].T
        left = wide_dot(roots[which], grad[:, lanes], ((1,), (0,)))
        gram = wide_dot(turn[...], grad[:, lanes], ((1,), (0,)))
        for head in range(heads):
            at = slice(head * HEAD, (head + 1) * HEAD)
            k_ref[which, head] = gram[at, at]
            pre_ref[which, :, at] = wide_dot(
                to_bf16(left[:, at]), col_roots[which, head], ((1,), (0,))
            )

    def travel(op):
        phase = int(op[1])
        if op[0] == "w" or phase == 2:
            landed(*piece(phase, op[2:] or "Ac"))
        forward(phase, op[2:] or "Ac")

    for op in PROGRAM:
        kind, rest = op[0], op[1:]
        if isinstance(op, tuple):
            gradients(int(op[0][1]), op[0][2:], op[1:])
        elif kind in "ow":
            travel(op)
        elif kind == "C":
            cotangents()
        elif kind == "T":
            from_core(rest)
            transpose(rest)
        elif kind == "S":
            first, last = int(rest[0]), int(rest[1])
            outer_step(slice(first * width, (last + 1) * width), first == 0, last == 3)
        elif kind == "L":
            for load in loads[5:9]:
                load.wait()
        elif kind == "P":
            products(pc, slice(2 * width, 3 * width))
        elif kind == "Q":
            products(1 - pc, slice(4 * width, 5 * width))

    dones[0].wait()
    mine_sum, their_sum = norms[0, 0:1, 0:1], norms[1, 0:1, 0:1]
    sums = (
        jnp.where(pc == 0, mine_sum, their_sum),
        jnp.where(pc == 0, their_sum, mine_sum),
    )
    for which in range(2):
        scale_twice = size / (sums[which] + 1.0)
        pre_ref[which] = pre_ref[which] * jnp.sqrt(scale_twice)
        for head in range(heads):
            k_ref[which, head] = k_ref[which, head] * (
                (1.0 - stat_decay) / features * scale_twice
            )
    for step in dones[1:]:
        outer_copy(pc, step).wait_send()
        outer_copy(1 - pc, step).wait_recv()
    for cond, build in pending:
        guarded(cond, lambda build=build: build().wait_send())


def in_hbm(*arrays):
    return [pltpu.with_memory_space_constraint(array, pltpu.HBM) for array in arrays]


def relayed_products(x, query_grad, forget_grad, forget_pre, lower_bound, *held):
    shards, parts = lax.axis_size("fs"), lax.axis_size("tp")
    block, span = x.shape
    width = query_grad.shape[1]
    chunk, features = held[0].shape
    bf16, f32 = jnp.bfloat16, jnp.float32
    heads = held[2].shape
    vmem = pl.BlockSpec(memory_space=pltpu.VMEM)
    hbm = pl.BlockSpec(memory_space=pltpu.HBM)
    return pl.pallas_call(
        relay_kernel,
        out_shape=[
            pltpu.VMEM((2, chunk, features), bf16),
            pltpu.VMEM((2, chunk, width), f32),
            pltpu.VMEM((2,) + heads, f32),
            pltpu.VMEM((2, chunk, width), f32),
            pltpu.VMEM((2, chunk, width), f32),
            pltpu.VMEM((2, chunk, features), f32),
            pltpu.VMEM((2,) + heads, f32),
        ],
        in_specs=[hbm] * 17,
        out_specs=[vmem] * 7,
        scratch_shapes=[
            pltpu.VMEM((shards, parts, block, span), bf16),
            pltpu.VMEM((shards, 2, 2, block, width), bf16),
            pltpu.VMEM((shards, block, width), bf16),
            pltpu.VMEM((features, shards * block), bf16),
            pltpu.VMEM((parts + 1, features, width), f32),
            pltpu.VMEM((features, (parts + 1) * width), bf16),
            pltpu.VMEM((chunk, features), f32),
            pltpu.VMEM((2, 8, 128), f32),
            pltpu.VMEM((2, chunk, features), bf16),
            pltpu.VMEM((2,) + heads, bf16),
            pltpu.VMEM((3, block, width), bf16),
            pltpu.VMEM((1, width), f32),
            pltpu.VMEM((width, features), bf16),
            pltpu.SemaphoreType.DMA((17,)),
            pltpu.SemaphoreType.DMA((128,)),
            pltpu.SemaphoreType.DMA((2, shards, parts)),
            pltpu.SemaphoreType.DMA((2, shards, 2)),
            pltpu.SemaphoreType.DMA((shards,)),
            pltpu.SemaphoreType.DMA((10,)),
        ],
        compiler_params=pltpu.CompilerParams(
            collective_id=0, has_side_effects=True, vmem_limit_bytes=48 * 1024 * 1024
        ),
    )(
        *in_hbm(x, query_grad, forget_grad, forget_pre, lower_bound.reshape(1, -1), *held)
    )


def finish_kernel(outer_ref, pre_ref, column_ref, weight_ref, moment_ref, rows_ref, cols_ref, *outs):
    step = pl.program_id(0)
    tile, head_tile = outs[0].shape[0], outs[10].shape[1]
    at = pl.ds(pl.multiple_of(step * tile, tile), tile)
    head_at = pl.ds(pl.multiple_of(step * head_tile, head_tile), head_tile)
    for which in range(2):
        master_out, copy_out, step_out, moment_out, rows_out, cols_out = outs[which::2]
        precond = pre_ref[which, at, :]
        moment_next = moment_decay * moment_ref[which, at, :] + (1.0 - moment_decay) * precond
        update_step = moment_decay * moment_next + (1.0 - moment_decay) * precond
        master = weight_ref[which, at, :] - learn_rate * update_step
        master_out[...] = master
        copy_out[...] = to_bf16(master)
        step_out[...] = update_step
        moment_out[...] = moment_next
        rows_out[...] = stat_decay * rows_ref[which, at, :] + outer_ref[which, at, :].astype(
            jnp.float32
        )
        cols_out[...] = (
            stat_decay * cols_ref[which, :, head_at, :] + column_ref[which, :, head_at, :]
        )


def finished(held):
    f32, bf16 = jnp.float32, jnp.bfloat16
    _, chunk, features = held[0].shape
    width = held[1].shape[2]
    heads = held[2].shape[1:]
    steps = 4
    tile = chunk // steps
    narrow = pl.BlockSpec((tile, width), lambda i: (i, 0))
    wide = pl.BlockSpec((tile, features), lambda i: (i, 0))
    head = pl.BlockSpec((heads[0], heads[1] // steps, heads[2]), lambda i: (0, i, 0))
    flat = lambda kind: [jax.ShapeDtypeStruct((chunk, width), kind)] * 2
    return pl.pallas_call(
        finish_kernel,
        grid=(steps,),
        out_shape=flat(f32)
        + flat(bf16)
        + flat(f32)
        + flat(f32)
        + [jax.ShapeDtypeStruct((chunk, features), f32)] * 2
        + [jax.ShapeDtypeStruct(heads, f32)] * 2,
        in_specs=[pl.BlockSpec(memory_space=pltpu.VMEM)] * 7,
        out_specs=[narrow] * 8 + [wide] * 2 + [head] * 2,
        compiler_params=pltpu.CompilerParams(vmem_limit_bytes=24 * 1024 * 1024),
    )(*[pltpu.with_memory_space_constraint(array, pltpu.VMEM) for array in held])


def gather_plan(
    inputs,
    query_grad,
    forget_grad,
    forget_pre,
    lower_bound,
    query_weight,
    forget_weight,
    query_moment,
    forget_moment,
    query_rows,
    forget_rows,
    query_cols,
    forget_cols,
    query_row_root,
    forget_row_root,
    query_col_root,
    forget_col_root,
):
    held = relayed_products(
        inputs,
        query_grad,
        forget_grad,
        forget_pre,
        lower_bound,
        query_row_root,
        forget_row_root,
        query_col_root,
        forget_col_root,
        query_weight,
        forget_weight,
        query_moment,
        forget_moment,
        query_rows,
        forget_rows,
        query_cols,
        forget_cols,
    )
    return tuple(finished(held))


def on_device(*args):
    token_count = args[0].shape[0] * lax.axis_size("fs")
    feature_count = args[0].shape[1] * lax.axis_size("tp")
    paired = lax.axis_size("fs") == 8 and lax.axis_size("tp") == 4
    if paired and token_count <= feature_count:
        return gather_plan(*args)
    return reduce_plan(*args)


def solution(mesh):
    in_specs = (
        P("fs", "tp"),
        P("fs", "tp"),
        P("fs", "tp"),
        P("fs", "tp"),
        P("tp"),
        P("fs", "tp"),
        P("fs", "tp"),
        P("fs", "tp"),
        P("fs", "tp"),
        P("fs", None),
        P("fs", None),
        P("tp", None, None),
        P("tp", None, None),
        P("fs", None),
        P("fs", None),
        P("tp", None, None),
        P("tp", None, None),
    )
    out_specs = (
        P("fs", "tp"),
        P("fs", "tp"),
        P("fs", "tp"),
        P("fs", "tp"),
        P("fs", "tp"),
        P("fs", "tp"),
        P("fs", "tp"),
        P("fs", "tp"),
        P("fs", None),
        P("fs", None),
        P("tp", None, None),
        P("tp", None, None),
    )
    return jax.shard_map(
        on_device, mesh=mesh, in_specs=in_specs, out_specs=out_specs, check_vma=False
    )
```

```python
import jax
import jax.numpy as jnp
from jax import lax
from jax.experimental import pallas as pl
from jax.experimental.pallas import tpu as pltpu
from jax.sharding import PartitionSpec as P

D = 2048
HW = 1024
HEAD = 128


stat_decay = 0.9
moment_decay = 0.9
learn_rate = 0.02
highest = lax.Precision.HIGHEST
MESH = pl.DeviceIdType.MESH


def fold_one(carry_state, shard_piece, offset, root_mine, grad_mine):
    left_sum, outer_rows, column_total = carry_state
    row_count, col_width = shard_piece.shape
    left_sum = left_sum + jnp.dot(root_mine, shard_piece, precision=highest)
    outer_piece = lax.dot_general(
        grad_mine, shard_piece, (((1,), (1,)), ((), ())), precision=highest
    )
    outer_rows = lax.dynamic_update_slice_in_dim(outer_rows, outer_piece, offset, 1)
    by_head = shard_piece.reshape(row_count, col_width // HEAD, HEAD)
    column_total = column_total + jnp.einsum("rhi,rhj->hij", by_head, by_head, precision=highest)
    return (left_sum, outer_rows, column_total)


def finish(weight, moment, rows, cols, col_root, left_sum, outer_rows, column_total, square):
    norm_scale = jnp.sqrt(D * HW / (square + 1.0))
    scale_twice = norm_scale * norm_scale
    rows_next = stat_decay * rows + (1.0 - stat_decay) / HW * scale_twice * outer_rows
    cols_next = stat_decay * cols + (1.0 - stat_decay) / D * scale_twice * column_total
    shard_rows, col_width = left_sum.shape
    shaped = left_sum.reshape(shard_rows, col_width // HEAD, HEAD)
    precond = norm_scale * jnp.einsum(
        "rhi,hij->rhj", shaped, col_root.astype(jnp.float32), precision=highest
    ).reshape(shard_rows, col_width)
    moment_next = moment_decay * moment + (1.0 - moment_decay) * precond
    update_step = moment_decay * moment_next + (1.0 - moment_decay) * precond
    master = weight - learn_rate * update_step
    return (master, master.astype(jnp.bfloat16), update_step, moment_next, rows_next, cols_next)


def reduce_plan(
    inputs,
    query_grad,
    forget_grad,
    forget_pre,
    lower_bound,
    query_weight,
    forget_weight,
    query_moment,
    forget_moment,
    query_rows,
    forget_rows,
    query_cols,
    forget_cols,
    query_row_root,
    forget_row_root,
    query_col_root,
    forget_col_root,
):
    sigma_gate = jax.nn.sigmoid(forget_pre.astype(jnp.float32))
    forget_cot = (
        forget_grad.astype(jnp.float32) * (1.0 - lower_bound) * sigma_gate * (1.0 - sigma_gate)
    ).astype(jnp.bfloat16)
    gathered = lax.all_gather(inputs, "tp", axis=1, tiled=True)
    shard_rows, col_width = query_weight.shape
    heads_here = col_width // HEAD
    row_roots = (query_row_root.astype(jnp.float32), forget_row_root.astype(jnp.float32))
    empty = (
        jnp.zeros((shard_rows, col_width), jnp.float32),
        jnp.zeros((shard_rows, D), jnp.float32),
        jnp.zeros((heads_here, HEAD, HEAD), jnp.float32),
    )
    joined = jnp.concatenate([query_grad, forget_cot], axis=1)
    summed = lax.psum_scatter(
        lax.dot_general(
            gathered, joined, (((0,), (0,)), ((), ())), preferred_element_type=jnp.float32
        ),
        "fs",
        scatter_dimension=0,
        tiled=True,
    )
    gradients = (summed[:, :col_width], summed[:, col_width:])
    offset = jnp.int32(0)
    results = (
        fold_one(
            empty,
            lax.all_gather(gradients[0].astype(jnp.bfloat16), "fs", axis=0, tiled=True).astype(
                jnp.float32
            ),
            offset,
            row_roots[0],
            gradients[0],
        ),
        fold_one(
            empty,
            lax.all_gather(gradients[1].astype(jnp.bfloat16), "fs", axis=0, tiled=True).astype(
                jnp.float32
            ),
            offset,
            row_roots[1],
            gradients[1],
        ),
    )
    query_trace = jnp.sum(jnp.diagonal(results[0][2], axis1=1, axis2=2))
    forget_trace = jnp.sum(jnp.diagonal(results[1][2], axis1=1, axis2=2))
    query_outer, forget_outer, query_square, forget_square = (
        lax.psum(results[0][1].astype(jnp.bfloat16), "tp").astype(jnp.float32),
        lax.psum(results[1][1].astype(jnp.bfloat16), "tp").astype(jnp.float32),
        lax.psum(query_trace.astype(jnp.bfloat16), "tp").astype(jnp.float32),
        lax.psum(forget_trace.astype(jnp.bfloat16), "tp").astype(jnp.float32),
    )
    query_out = finish(
        query_weight,
        query_moment,
        query_rows,
        query_cols,
        query_col_root,
        results[0][0],
        query_outer,
        results[0][2],
        query_square,
    )
    forget_out = finish(
        forget_weight,
        forget_moment,
        forget_rows,
        forget_cols,
        forget_col_root,
        results[1][0],
        forget_outer,
        results[1][2],
        forget_square,
    )
    return (
        query_out[0],
        forget_out[0],
        query_out[1],
        forget_out[1],
        query_out[2],
        forget_out[2],
        query_out[3],
        forget_out[3],
        query_out[4],
        forget_out[4],
        query_out[5],
        forget_out[5],
    )


def to_bf16(value):
    return value.astype(jnp.bfloat16)


def wide_dot(left, right, dims):
    return lax.dot_general(left, right, (dims, ((), ())), preferred_element_type=jnp.float32)


LAYERS = "ACDB"
ROUTES = {
    "Ac": ("b", "m", "p", "s"),
    "Bc": ("m", "s"),
    "Cc": ("n", "p", "s"),
    "Dc": ("n", "p", "s"),
    "Ap": ("s", "b"),
    "Cp": ("s",),
    "Dp": ("s",),
    "Ad": ("b",),
}
PROGRAM = (
    "o0", "o1", "C", "o2", "w0Ap", "w1Bc", "o3", "w2Bc", "w0Bc", "w0Cc", "w2Cc", "w0Bp", "w1Cc",
    "w1Dc", "w1Ap", "w0Cp", "w1As", "w0Dc", "w3Bc", "w2Cp", "w2Ap", "w1Ds", "w1Dp", "w0Cs",
    "w2Dc", "w0Cd", "w0Bs", "w1Ad", "w1Cp", "w0Ad", "w2Cd", "w0Ds", "w1Bs", "w0Dp", "w2Bp",
    "w1Bp", "w3Ap", "w1Cs", "w0As", "TA", "w2Dp", "w3Cc", "w2As", "w1Dd", "w3Dc", "w3Bp", "w3Bs",
    "w2Cs", "w0Dd", "w3Ad", "w2Ds", "w0Bd", "w2Ad", "w1Cd", "w1Bd", "TD", "w2Dd", "TC", "w3Cp",
    "w2Bs", ("GACD", (), ("w3As", "w3Dp", "w3Bd",)), "TB", "w2Bd",
    ("GB", (), ("w3Ds", "w3Cs", "w3Cd", "w3Dd",)), "S01", "L", "Q", ("HACD",), ("HB",), "S23",
    "P",
)

BLOCKS = {"G": (2, (0, 1, 2), 4), "H": (3, (0, 1), 4)}


def relay_kernel(
    x_hbm, q_hbm, g_hbm, pre_hbm, bound_hbm, rq_hbm, rf_hbm, cq_hbm, cf_hbm,
    wq_hbm, wf_hbm, mq_hbm, mf_hbm, hq_hbm, hf_hbm, vq_hbm, vf_hbm,
    s_ref, pre_ref, k_ref, weight_ref, moment_ref, rows_ref, cols_ref,
    xs, gs, go, xt, acc, grad, sacc, norms, roots, col_roots, raw, bound, turn,
    own_sem, send_sem, x_sem, g_sem, o_sem, swap_sem,
):
    shards, parts, block, span = xs.shape
    width = go.shape[2]
    features = xt.shape[0]
    chunk = s_ref.shape[1]
    heads = width // HEAD
    f32 = jnp.float32
    fs = lax.axis_index("fs")
    tp = lax.axis_index("tp")
    z, px = lax.div(fs, 2), lax.rem(fs, 2)
    py, pc = lax.div(tp, 2), lax.rem(tp, 2)
    pair = z + 1 - 2 * lax.rem(z, 2)
    low = z < 2
    near = jnp.where(low, 2, 1)
    layer = {"A": z, "B": pair, "C": near, "D": jnp.where(low, 3, 0)}
    middle = jnp.logical_and(z > 0, z < 3)
    flips = {"c": (0, 0), "p": (1 - pc, pc), "s": (pc, 1 - pc), "d": (1, 1)}

    def column(who):
        flip_x, flip_y = flips[who]
        return px + flip_x - 2 * px * flip_x, py + flip_y - 2 * py * flip_y

    def device(link):
        if link in ("b", "n"):
            return (2 * pair + px, tp)
        if link == "m":
            return (2 * near + px, tp)
        if link == "core":
            return (fs, tp + 1 - 2 * pc)
        x, y = column(link)
        return (2 * z + x, 2 * y + pc)

    beside = {link: device(link) for link in ("b", "n", "m", "p", "s", "core")}
    conds = {"n": middle, "m": middle}
    aside = {"c": None, "p": pc == 0, "s": pc == 1}

    def guarded(cond, action):
        if cond is None:
            action()
        else:
            pl.when(cond)(action)

    barrier = pltpu.get_barrier_semaphore()

    def greet(name):
        pl.semaphore_signal(barrier, inc=1, device_id=beside[name], device_id_type=MESH)

    for name in ("b", "p", "s", "core"):
        greet(name)
    guarded(middle, lambda: greet("m"))
    loads = [
        pltpu.make_async_copy(source, target, own_sem.at[number])
        for number, (source, target) in enumerate(
            (
                (x_hbm, xs.at[fs, tp]),
                (q_hbm, raw.at[0]),
                (g_hbm, raw.at[1]),
                (pre_hbm, raw.at[2]),
                (bound_hbm, bound),
                (rq_hbm, roots.at[0]),
                (rf_hbm, roots.at[1]),
                (cq_hbm, col_roots.at[0]),
                (cf_hbm, col_roots.at[1]),
                (wq_hbm, weight_ref.at[0]),
                (wf_hbm, weight_ref.at[1]),
                (mq_hbm, moment_ref.at[0]),
                (mf_hbm, moment_ref.at[1]),
                (hq_hbm, rows_ref.at[0]),
                (hf_hbm, rows_ref.at[1]),
                (vq_hbm, cols_ref.at[0]),
                (vf_hbm, cols_ref.at[1]),
            )
        )
    ]
    for load in loads[:5]:
        load.start()
    loads[0].wait()
    pl.semaphore_wait(barrier, 4 + jnp.where(middle, 1, 0))

    def cotangents():
        for load in loads[1:5]:
            load.wait()
        sigma_gate = jax.nn.sigmoid(raw[2].astype(f32))
        cot = to_bf16(
            raw[1].astype(f32) * (1.0 - bound[...]) * sigma_gate * (1.0 - sigma_gate)
        )

        @pl.when(pc == 0)
        def _():
            gs[fs, py, 0] = raw[0]
            go[fs] = cot

        @pl.when(pc == 1)
        def _():
            gs[fs, py, 1] = cot
            go[fs] = raw[0]

        for load in loads[5:]:
            load.start()
        start(lambda: (go.at[fs], gs.at[fs, py, pc], g_sem.at[0, fs, py]), "core")

    half_rows = block // 2
    pending = []
    dones = []

    def halves(phase):
        return 1 - pc if phase == 2 else pc

    def piece(phase, name):
        x, y = column(name[1])
        shard = 2 * layer[name[0]] + x
        if phase < 2:
            rows = pl.ds(phase * half_rows, half_rows)
            part = 2 * y + pc
            return xs.at[shard, part, rows], x_sem.at[phase, shard, part]
        return gs.at[shard, y, halves(phase)], g_sem.at[phase - 2, shard, y]

    def start(recipe, link, cond=None):
        number = len(pending)

        def build():
            src, dst, sem = recipe()
            return pltpu.make_async_remote_copy(
                src_ref=src, dst_ref=dst, send_sem=send_sem.at[number], recv_sem=sem,
                device_id=beside[link], device_id_type=MESH,
            )

        guarded(cond, lambda: build().start())
        pending.append((cond, build))

    def landed(ref, sem):
        pltpu.make_async_remote_copy(
            src_ref=ref, dst_ref=ref, send_sem=send_sem.at[0], recv_sem=sem,
            device_id=beside["core"], device_id_type=MESH,
        ).wait_recv()

    def forward(phase, name):
        def same():
            here, sem = piece(phase, name)
            return here, here, sem

        def beyond():
            here, _ = piece(phase, name)
            shard = 2 * layer[name[0]] + column(name[1])[0]
            return here, go.at[shard], o_sem.at[shard]

        for link in ROUTES.get(name, ()):
            start(same, link, conds.get(link))
        if phase < 2:
            start(same, "core")
        if phase == 2 and name != "Ac" and name[1] != "d":
            start(beyond, "core", aside[name[1]])

    def from_core(label):
        for phase in range(2):
            for x in range(2):
                for y in range(2):
                    shard, part = 2 * layer[label] + x, 2 * y + 1 - pc
                    rows = pl.ds(phase * half_rows, half_rows)
                    landed(xs.at[shard, part, rows], x_sem.at[phase, shard, part])

    def transpose(label):
        at = LAYERS.index(label)

        @pl.loop(0, 2)
        def _(x):
            lanes = pl.ds(pl.multiple_of((2 * at + x) * block, block), block)
            for part in range(parts):
                turned = xs[2 * layer[label] + x, part].T
                xt[part * span : (part + 1) * span, lanes] = turned

    squares = []

    def own_block(phase, far, label):
        y = 1 - py if far else py
        both = pl.ds(2 * layer[label], 2)
        return gs[both, y, halves(phase)].reshape(2 * block, width)

    def other_block(label):
        return go[pl.ds(2 * layer[label], 2)].reshape(2 * block, width)

    def gradients(phase, fars, tiles, labels, events):
        tile = features // tiles
        first, final = labels[0] == LAYERS[0], labels[-1] == LAYERS[-1]
        start_token = LAYERS.index(labels[0]) * 2 * block
        tokens = slice(start_token, start_token + len(labels) * 2 * block)
        if phase == 2:
            for label in labels:
                for x in range(2):
                    shard = 2 * layer[label] + x
                    guarded(
                        px != x if label == "A" else None,
                        lambda shard=shard: landed(go.at[shard], o_sem.at[shard]),
                    )

        def body(step, total):
            rows = pl.ds(pl.multiple_of(step * tile, tile), tile)
            for far in fars:
                at = 4 if far == 2 else 2 * (phase - 2) + far
                right = jnp.concatenate(
                    [other_block(k) if far == 2 else own_block(phase, far, k) for k in labels], axis=0
                )
                value = wide_dot(xt[rows, tokens], right, ((1,), (0,)))
                if not first:
                    value = value + acc[at, rows, :]
                if final:
                    grad[rows, at * width : (at + 1) * width] = to_bf16(value)
                    if far < 2:
                        squared = (value * value).reshape(tile // 8, 8, width)
                        total = total + jnp.sum(squared, axis=0)
                else:
                    acc[at, rows, :] = value
            for number, names in enumerate(events):
                if names:

                    @pl.when(step == number)
                    def _(names=names):
                        for name in names:
                            travel(name)

            return total

        total = lax.fori_loop(0, features // tile, body, jnp.zeros((8, width), f32))
        if final:
            squares.append(total)

    mine = pl.ds(pl.multiple_of(fs * chunk, chunk), chunk)
    hidden = parts * width
    size = float(features * hidden)

    def outer_step(lanes, first, final):
        wide = 2 * chunk
        if final:
            square = jnp.sum(squares[0], axis=(0, 1), keepdims=True)
            for more in squares[1:]:
                square = square + jnp.sum(more, axis=(0, 1), keepdims=True)
            norms[0] = jnp.broadcast_to(square, norms.shape[1:])
            scale = (1.0 - stat_decay) / hidden * (size / (square + 1.0))
            swap_norm = pltpu.make_async_remote_copy(
                src_ref=norms.at[0], dst_ref=norms.at[1],
                send_sem=swap_sem.at[0], recv_sem=swap_sem.at[1],
                device_id=beside["core"], device_id_type=MESH,
            )
        if not final:

            broad = 2 * wide

            @pl.loop(0, features // broad)
            def _(step):
                rows = pl.ds(pl.multiple_of(step * broad, broad), broad)
                product = wide_dot(grad[mine, lanes], grad[rows, lanes], ((1,), (1,)))
                if not first:
                    product = product + sacc[:, rows]
                sacc[:, rows] = product

            return
        for step in range(features // wide):
            rows = slice(step * wide, (step + 1) * wide)
            product = wide_dot(grad[mine, lanes], grad[rows, lanes], ((1,), (1,)))
            s_ref[pc, :, rows] = to_bf16((product + sacc[:, rows]) * scale)
            if step == 0:
                swap_norm.start()
                dones.append(swap_norm)
            else:
                send_outer(step - 1)
        for load in loads[9:]:
            load.wait()
        send_outer(features // wide - 1)

    def outer_copy(which, step):
        rows = pl.ds(step * 2 * chunk, 2 * chunk)
        return pltpu.make_async_remote_copy(
            src_ref=s_ref.at[which, :, rows], dst_ref=s_ref.at[which, :, rows],
            send_sem=swap_sem.at[2 + step], recv_sem=swap_sem.at[6 + step],
            device_id=beside["core"], device_id_type=MESH,
        )

    def send_outer(step):
        outer_copy(pc, step).start()
        dones.append(step)

    def products(which, lanes):
        for step in range(features // chunk):
            rows = slice(step * chunk, (step + 1) * chunk)
            turn[:, rows] = grad[rows, lanes].T
        left = wide_dot(roots[which], grad[:, lanes], ((1,), (0,)))
        gram = wide_dot(turn[...], grad[:, lanes], ((1,), (0,)))
        for head in range(heads):
            at = slice(head * HEAD, (head + 1) * HEAD)
            k_ref[which, head] = gram[at, at]
            pre_ref[which, :, at] = wide_dot(
                to_bf16(left[:, at]), col_roots[which, head], ((1,), (0,))
            )

    def travel(op):
        phase = int(op[1])
        if op[0] == "w" or phase == 2:
            landed(*piece(phase, op[2:] or "Ac"))
        forward(phase, op[2:] or "Ac")

    for op in PROGRAM:
        kind, rest = op[0], op[1:]
        if isinstance(op, tuple):
            gradients(*BLOCKS[op[0][0]], op[0][1:], op[1:])
        elif kind in "ow":
            travel(op)
        elif kind == "C":
            cotangents()
        elif kind == "T":
            from_core(rest)
            transpose(rest)
        elif kind == "S":
            first, last = int(rest[0]), int(rest[1])
            outer_step(slice(first * width, (last + 1) * width), first == 0, last == 3)
        elif kind == "L":
            for load in loads[5:9]:
                load.wait()
        elif kind == "P":
            products(pc, slice(2 * width, 3 * width))
        elif kind == "Q":
            products(1 - pc, slice(4 * width, 5 * width))

    dones[0].wait()
    mine_sum, their_sum = norms[0, 0:1, 0:1], norms[1, 0:1, 0:1]
    sums = (
        jnp.where(pc == 0, mine_sum, their_sum),
        jnp.where(pc == 0, their_sum, mine_sum),
    )
    for which in range(2):
        scale_twice = size / (sums[which] + 1.0)
        pre_ref[which] = pre_ref[which] * jnp.sqrt(scale_twice)
        for head in range(heads):
            k_ref[which, head] = k_ref[which, head] * (
                (1.0 - stat_decay) / features * scale_twice
            )
    for cond, build in pending:
        guarded(cond, lambda build=build: build().wait_send())
    for step in dones[1:]:
        outer_copy(pc, step).wait_send()
        outer_copy(1 - pc, step).wait_recv()


def in_hbm(*arrays):
    return [pltpu.with_memory_space_constraint(array, pltpu.HBM) for array in arrays]


def relayed_products(x, query_grad, forget_grad, forget_pre, lower_bound, *held):
    shards, parts = lax.axis_size("fs"), lax.axis_size("tp")
    block, span = x.shape
    width = query_grad.shape[1]
    chunk, features = held[0].shape
    bf16, f32 = jnp.bfloat16, jnp.float32
    heads = held[2].shape
    vmem = pl.BlockSpec(memory_space=pltpu.VMEM)
    hbm = pl.BlockSpec(memory_space=pltpu.HBM)
    return pl.pallas_call(
        relay_kernel,
        out_shape=[
            pltpu.VMEM((2, chunk, features), bf16),
            pltpu.VMEM((2, chunk, width), f32),
            pltpu.VMEM((2,) + heads, f32),
            pltpu.VMEM((2, chunk, width), f32),
            pltpu.VMEM((2, chunk, width), f32),
            pltpu.VMEM((2, chunk, features), f32),
            pltpu.VMEM((2,) + heads, f32),
        ],
        in_specs=[hbm] * 17,
        out_specs=[vmem] * 7,
        scratch_shapes=[
            pltpu.VMEM((shards, parts, block, span), bf16),
            pltpu.VMEM((shards, 2, 2, block, width), bf16),
            pltpu.VMEM((shards, block, width), bf16),
            pltpu.VMEM((features, shards * block), bf16),
            pltpu.VMEM((parts + 1, features, width), f32),
            pltpu.VMEM((features, (parts + 1) * width), bf16),
            pltpu.VMEM((chunk, features), f32),
            pltpu.VMEM((2, 8, 128), f32),
            pltpu.VMEM((2, chunk, features), bf16),
            pltpu.VMEM((2,) + heads, bf16),
            pltpu.VMEM((3, block, width), bf16),
            pltpu.VMEM((1, width), f32),
            pltpu.VMEM((width, features), bf16),
            pltpu.SemaphoreType.DMA((17,)),
            pltpu.SemaphoreType.DMA((128,)),
            pltpu.SemaphoreType.DMA((2, shards, parts)),
            pltpu.SemaphoreType.DMA((2, shards, 2)),
            pltpu.SemaphoreType.DMA((shards,)),
            pltpu.SemaphoreType.DMA((10,)),
        ],
        compiler_params=pltpu.CompilerParams(
            collective_id=0, has_side_effects=True, vmem_limit_bytes=48 * 1024 * 1024
        ),
    )(
        *in_hbm(x, query_grad, forget_grad, forget_pre, lower_bound.reshape(1, -1), *held)
    )


def finish_kernel(outer_ref, pre_ref, column_ref, weight_ref, moment_ref, rows_ref, cols_ref, *outs):
    step = pl.program_id(0)
    tile, head_tile = outs[0].shape[0], outs[10].shape[1]
    at = pl.ds(pl.multiple_of(step * tile, tile), tile)
    head_at = pl.ds(pl.multiple_of(step * head_tile, head_tile), head_tile)
    for which in range(2):
        master_out, copy_out, step_out, moment_out, rows_out, cols_out = outs[which::2]
        precond = pre_ref[which, at, :]
        moment_next = moment_decay * moment_ref[which, at, :] + (1.0 - moment_decay) * precond
        update_step = moment_decay * moment_next + (1.0 - moment_decay) * precond
        master = weight_ref[which, at, :] - learn_rate * update_step
        master_out[...] = master
        copy_out[...] = to_bf16(master)
        step_out[...] = update_step
        moment_out[...] = moment_next
        rows_out[...] = stat_decay * rows_ref[which, at, :] + outer_ref[which, at, :].astype(
            jnp.float32
        )
        cols_out[...] = (
            stat_decay * cols_ref[which, :, head_at, :] + column_ref[which, :, head_at, :]
        )


def finished(held):
    f32, bf16 = jnp.float32, jnp.bfloat16
    _, chunk, features = held[0].shape
    width = held[1].shape[2]
    heads = held[2].shape[1:]
    steps = 4
    tile = chunk // steps
    narrow = pl.BlockSpec((tile, width), lambda i: (i, 0))
    wide = pl.BlockSpec((tile, features), lambda i: (i, 0))
    head = pl.BlockSpec((heads[0], heads[1] // steps, heads[2]), lambda i: (0, i, 0))
    flat = lambda kind: [jax.ShapeDtypeStruct((chunk, width), kind)] * 2
    return pl.pallas_call(
        finish_kernel,
        grid=(steps,),
        out_shape=flat(f32)
        + flat(bf16)
        + flat(f32)
        + flat(f32)
        + [jax.ShapeDtypeStruct((chunk, features), f32)] * 2
        + [jax.ShapeDtypeStruct(heads, f32)] * 2,
        in_specs=[pl.BlockSpec(memory_space=pltpu.VMEM)] * 7,
        out_specs=[narrow] * 8 + [wide] * 2 + [head] * 2,
        compiler_params=pltpu.CompilerParams(vmem_limit_bytes=24 * 1024 * 1024),
    )(*[pltpu.with_memory_space_constraint(array, pltpu.VMEM) for array in held])


def gather_plan(
    inputs,
    query_grad,
    forget_grad,
    forget_pre,
    lower_bound,
    query_weight,
    forget_weight,
    query_moment,
    forget_moment,
    query_rows,
    forget_rows,
    query_cols,
    forget_cols,
    query_row_root,
    forget_row_root,
    query_col_root,
    forget_col_root,
):
    held = relayed_products(
        inputs,
        query_grad,
        forget_grad,
        forget_pre,
        lower_bound,
        query_row_root,
        forget_row_root,
        query_col_root,
        forget_col_root,
        query_weight,
        forget_weight,
        query_moment,
        forget_moment,
        query_rows,
        forget_rows,
        query_cols,
        forget_cols,
    )
    return tuple(finished(held))


def on_device(*args):
    token_count = args[0].shape[0] * lax.axis_size("fs")
    feature_count = args[0].shape[1] * lax.axis_size("tp")
    paired = lax.axis_size("fs") == 8 and lax.axis_size("tp") == 4
    if paired and token_count <= feature_count:
        return gather_plan(*args)
    return reduce_plan(*args)


def solution(mesh):
    in_specs = (
        P("fs", "tp"),
        P("fs", "tp"),
        P("fs", "tp"),
        P("fs", "tp"),
        P("tp"),
        P("fs", "tp"),
        P("fs", "tp"),
        P("fs", "tp"),
        P("fs", "tp"),
        P("fs", None),
        P("fs", None),
        P("tp", None, None),
        P("tp", None, None),
        P("fs", None),
        P("fs", None),
        P("tp", None, None),
        P("tp", None, None),
    )
    out_specs = (
        P("fs", "tp"),
        P("fs", "tp"),
        P("fs", "tp"),
        P("fs", "tp"),
        P("fs", "tp"),
        P("fs", "tp"),
        P("fs", "tp"),
        P("fs", "tp"),
        P("fs", None),
        P("fs", None),
        P("tp", None, None),
        P("tp", None, None),
    )
    return jax.shard_map(
        on_device, mesh=mesh, in_specs=in_specs, out_specs=out_specs, check_vma=False
    )
```

```python
import jax
import jax.numpy as jnp
from jax import lax
from jax.experimental import pallas as pl
from jax.experimental.pallas import tpu as pltpu
from jax.sharding import PartitionSpec as P

D = 2048
HW = 1024
HEAD = 128


stat_decay = 0.9
moment_decay = 0.9
learn_rate = 0.02
highest = lax.Precision.HIGHEST
MESH = pl.DeviceIdType.MESH


def fold_one(carry_state, shard_piece, offset, root_mine, grad_mine):
    left_sum, outer_rows, column_total = carry_state
    row_count, col_width = shard_piece.shape
    left_sum = left_sum + jnp.dot(root_mine, shard_piece, precision=highest)
    outer_piece = lax.dot_general(
        grad_mine, shard_piece, (((1,), (1,)), ((), ())), precision=highest
    )
    outer_rows = lax.dynamic_update_slice_in_dim(outer_rows, outer_piece, offset, 1)
    by_head = shard_piece.reshape(row_count, col_width // HEAD, HEAD)
    column_total = column_total + jnp.einsum("rhi,rhj->hij", by_head, by_head, precision=highest)
    return (left_sum, outer_rows, column_total)


def finish(weight, moment, rows, cols, col_root, left_sum, outer_rows, column_total, square):
    norm_scale = jnp.sqrt(D * HW / (square + 1.0))
    scale_twice = norm_scale * norm_scale
    rows_next = stat_decay * rows + (1.0 - stat_decay) / HW * scale_twice * outer_rows
    cols_next = stat_decay * cols + (1.0 - stat_decay) / D * scale_twice * column_total
    shard_rows, col_width = left_sum.shape
    shaped = left_sum.reshape(shard_rows, col_width // HEAD, HEAD)
    precond = norm_scale * jnp.einsum(
        "rhi,hij->rhj", shaped, col_root.astype(jnp.float32), precision=highest
    ).reshape(shard_rows, col_width)
    moment_next = moment_decay * moment + (1.0 - moment_decay) * precond
    update_step = moment_decay * moment_next + (1.0 - moment_decay) * precond
    master = weight - learn_rate * update_step
    return (master, master.astype(jnp.bfloat16), update_step, moment_next, rows_next, cols_next)


def reduce_plan(
    inputs,
    query_grad,
    forget_grad,
    forget_pre,
    lower_bound,
    query_weight,
    forget_weight,
    query_moment,
    forget_moment,
    query_rows,
    forget_rows,
    query_cols,
    forget_cols,
    query_row_root,
    forget_row_root,
    query_col_root,
    forget_col_root,
):
    sigma_gate = jax.nn.sigmoid(forget_pre.astype(jnp.float32))
    forget_cot = (
        forget_grad.astype(jnp.float32) * (1.0 - lower_bound) * sigma_gate * (1.0 - sigma_gate)
    ).astype(jnp.bfloat16)
    gathered = lax.all_gather(inputs, "tp", axis=1, tiled=True)
    shard_rows, col_width = query_weight.shape
    heads_here = col_width // HEAD
    row_roots = (query_row_root.astype(jnp.float32), forget_row_root.astype(jnp.float32))
    empty = (
        jnp.zeros((shard_rows, col_width), jnp.float32),
        jnp.zeros((shard_rows, D), jnp.float32),
        jnp.zeros((heads_here, HEAD, HEAD), jnp.float32),
    )
    joined = jnp.concatenate([query_grad, forget_cot], axis=1)
    summed = lax.psum_scatter(
        lax.dot_general(
            gathered, joined, (((0,), (0,)), ((), ())), preferred_element_type=jnp.float32
        ),
        "fs",
        scatter_dimension=0,
        tiled=True,
    )
    gradients = (summed[:, :col_width], summed[:, col_width:])
    offset = jnp.int32(0)
    results = (
        fold_one(
            empty,
            lax.all_gather(gradients[0].astype(jnp.bfloat16), "fs", axis=0, tiled=True).astype(
                jnp.float32
            ),
            offset,
            row_roots[0],
            gradients[0],
        ),
        fold_one(
            empty,
            lax.all_gather(gradients[1].astype(jnp.bfloat16), "fs", axis=0, tiled=True).astype(
                jnp.float32
            ),
            offset,
            row_roots[1],
            gradients[1],
        ),
    )
    query_trace = jnp.sum(jnp.diagonal(results[0][2], axis1=1, axis2=2))
    forget_trace = jnp.sum(jnp.diagonal(results[1][2], axis1=1, axis2=2))
    query_outer, forget_outer, query_square, forget_square = (
        lax.psum(results[0][1].astype(jnp.bfloat16), "tp").astype(jnp.float32),
        lax.psum(results[1][1].astype(jnp.bfloat16), "tp").astype(jnp.float32),
        lax.psum(query_trace.astype(jnp.bfloat16), "tp").astype(jnp.float32),
        lax.psum(forget_trace.astype(jnp.bfloat16), "tp").astype(jnp.float32),
    )
    query_out = finish(
        query_weight,
        query_moment,
        query_rows,
        query_cols,
        query_col_root,
        results[0][0],
        query_outer,
        results[0][2],
        query_square,
    )
    forget_out = finish(
        forget_weight,
        forget_moment,
        forget_rows,
        forget_cols,
        forget_col_root,
        results[1][0],
        forget_outer,
        results[1][2],
        forget_square,
    )
    return (
        query_out[0],
        forget_out[0],
        query_out[1],
        forget_out[1],
        query_out[2],
        forget_out[2],
        query_out[3],
        forget_out[3],
        query_out[4],
        forget_out[4],
        query_out[5],
        forget_out[5],
    )


def to_bf16(value):
    return value.astype(jnp.bfloat16)


def wide_dot(left, right, dims):
    return lax.dot_general(left, right, (dims, ((), ())), preferred_element_type=jnp.float32)


LAYERS = "ACDB"
ROUTES = {
    "Ac": ("b", "m", "p", "s"),
    "Bc": ("m", "s"),
    "Cc": ("n", "p", "s"),
    "Dc": ("n", "p", "s"),
    "Ap": ("s", "b"),
    "Cp": ("s",),
    "Dp": ("s",),
    "Ad": ("b",),
}
PROGRAM = (
    "o0", "o1", "C", "o2", "w0Ap", "o3", "w1Bc", "w2Bc", "w0Bc", "w2Cc", "w0Cc", "w1Dc", "w1Cc",
    "w0Bp", "w1Ap", "w1As", "w0Cp", "w3Bc", "w0Dc", "w2Cp", "w1Dp", "w2Ap", "w1Ds", "w0Cs",
    "w2Dc", "w0Ad", "w0Dp", "w1Bs", "w0Cd", "w1Ad", "w0Bs", "w1Cp", "w2Cd", "w3Ap", "w2As",
    "w1Bp", "w0As", "w1Cs", "TA", "w2Bp", "w2Dp", "w0Ds", "w3Cc", "w1Dd", "w2Cs", "w3Dc", "w2Ds",
    "w0Dd", "w3Bp", "w0Bd", "w3Ad", "w1Cd", "w2Ad", "w1Bd", "TD", "TC", "w2Dd", "TB", "w3Cp",
    "w3Bs", "w3As", ("GACD", (), ("w3Dp",), ("w3Ds", "w2Bs",)), "w3Bd", "w2Bd",
    ("GB", (), (), ("w3Cs",)), "S01", "w3Cd", "w3Dd", "L", "Q", ("HACD",), ("HB",), "S23", "P",
)

BLOCKS = {"G": (2, (0, 1, 2), 4), "H": (3, (0, 1), 4)}


def relay_kernel(
    x_hbm, q_hbm, g_hbm, pre_hbm, bound_hbm, rq_hbm, rf_hbm, cq_hbm, cf_hbm,
    wq_hbm, wf_hbm, mq_hbm, mf_hbm, hq_hbm, hf_hbm, vq_hbm, vf_hbm,
    s_ref, pre_ref, k_ref, weight_ref, moment_ref, rows_ref, cols_ref,
    xs, gs, go, xt, acc, grad, sacc, norms, roots, col_roots, raw, bound, turn,
    own_sem, send_sem, x_sem, g_sem, o_sem, swap_sem,
):
    shards, parts, block, span = xs.shape
    width = go.shape[2]
    features = xt.shape[0]
    chunk = s_ref.shape[1]
    heads = width // HEAD
    f32 = jnp.float32
    fs = lax.axis_index("fs")
    tp = lax.axis_index("tp")
    z, px = lax.div(fs, 2), lax.rem(fs, 2)
    py, pc = lax.div(tp, 2), lax.rem(tp, 2)
    pair = z + 1 - 2 * lax.rem(z, 2)
    low = z < 2
    near = jnp.where(low, 2, 1)
    layer = {"A": z, "B": pair, "C": near, "D": jnp.where(low, 3, 0)}
    middle = jnp.logical_and(z > 0, z < 3)
    flips = {"c": (0, 0), "p": (1 - pc, pc), "s": (pc, 1 - pc), "d": (1, 1)}

    def column(who):
        flip_x, flip_y = flips[who]
        return px + flip_x - 2 * px * flip_x, py + flip_y - 2 * py * flip_y

    def device(link):
        if link in ("b", "n"):
            return (2 * pair + px, tp)
        if link == "m":
            return (2 * near + px, tp)
        if link == "core":
            return (fs, tp + 1 - 2 * pc)
        x, y = column(link)
        return (2 * z + x, 2 * y + pc)

    beside = {link: device(link) for link in ("b", "n", "m", "p", "s", "core")}
    conds = {"n": middle, "m": middle}
    aside = {"c": None, "p": pc == 0, "s": pc == 1}

    def guarded(cond, action):
        if cond is None:
            action()
        else:
            pl.when(cond)(action)

    barrier = pltpu.get_barrier_semaphore()

    def greet(name):
        pl.semaphore_signal(barrier, inc=1, device_id=beside[name], device_id_type=MESH)

    for name in ("b", "p", "s", "core"):
        greet(name)
    guarded(middle, lambda: greet("m"))
    loads = [
        pltpu.make_async_copy(source, target, own_sem.at[number])
        for number, (source, target) in enumerate(
            (
                (x_hbm, xs.at[fs, tp]),
                (q_hbm, raw.at[0]),
                (g_hbm, raw.at[1]),
                (pre_hbm, raw.at[2]),
                (bound_hbm, bound),
                (rq_hbm, roots.at[0]),
                (rf_hbm, roots.at[1]),
                (cq_hbm, col_roots.at[0]),
                (cf_hbm, col_roots.at[1]),
                (wq_hbm, weight_ref.at[0]),
                (wf_hbm, weight_ref.at[1]),
                (mq_hbm, moment_ref.at[0]),
                (mf_hbm, moment_ref.at[1]),
                (hq_hbm, rows_ref.at[0]),
                (hf_hbm, rows_ref.at[1]),
                (vq_hbm, cols_ref.at[0]),
                (vf_hbm, cols_ref.at[1]),
            )
        )
    ]
    for load in loads[:5]:
        load.start()
    loads[0].wait()
    pl.semaphore_wait(barrier, 4 + jnp.where(middle, 1, 0))

    def cotangents():
        for load in loads[1:5]:
            load.wait()
        sigma_gate = jax.nn.sigmoid(raw[2].astype(f32))
        cot = to_bf16(
            raw[1].astype(f32) * (1.0 - bound[...]) * sigma_gate * (1.0 - sigma_gate)
        )

        @pl.when(pc == 0)
        def _():
            gs[fs, py, 0] = raw[0]
            go[fs] = cot

        @pl.when(pc == 1)
        def _():
            gs[fs, py, 1] = cot
            go[fs] = raw[0]

        for load in loads[5:]:
            load.start()
        start(lambda: (go.at[fs], gs.at[fs, py, pc], g_sem.at[0, fs, py]), "core")

    half_rows = block // 2
    pending = []
    dones = []

    def halves(phase):
        return 1 - pc if phase == 2 else pc

    def piece(phase, name):
        x, y = column(name[1])
        shard = 2 * layer[name[0]] + x
        if phase < 2:
            rows = pl.ds(phase * half_rows, half_rows)
            part = 2 * y + pc
            return xs.at[shard, part, rows], x_sem.at[phase, shard, part]
        return gs.at[shard, y, halves(phase)], g_sem.at[phase - 2, shard, y]

    def start(recipe, link, cond=None):
        number = len(pending)

        def build():
            src, dst, sem = recipe()
            return pltpu.make_async_remote_copy(
                src_ref=src, dst_ref=dst, send_sem=send_sem.at[number], recv_sem=sem,
                device_id=beside[link], device_id_type=MESH,
            )

        guarded(cond, lambda: build().start())
        pending.append((cond, build))

    def landed(ref, sem):
        pltpu.make_async_remote_copy(
            src_ref=ref, dst_ref=ref, send_sem=send_sem.at[0], recv_sem=sem,
            device_id=beside["core"], device_id_type=MESH,
        ).wait_recv()

    def forward(phase, name):
        def same():
            here, sem = piece(phase, name)
            return here, here, sem

        def beyond():
            here, _ = piece(phase, name)
            shard = 2 * layer[name[0]] + column(name[1])[0]
            return here, go.at[shard], o_sem.at[shard]

        for link in ROUTES.get(name, ()):
            start(same, link, conds.get(link))
        if phase < 2:
            start(same, "core")
        if phase == 2 and name != "Ac" and name[1] != "d":
            start(beyond, "core", aside[name[1]])

    def from_core(label):
        for phase in range(2):
            for x in range(2):
                for y in range(2):
                    shard, part = 2 * layer[label] + x, 2 * y + 1 - pc
                    rows = pl.ds(phase * half_rows, half_rows)
                    landed(xs.at[shard, part, rows], x_sem.at[phase, shard, part])

    def transpose(label):
        at = LAYERS.index(label)

        @pl.loop(0, 2)
        def _(x):
            lanes = pl.ds(pl.multiple_of((2 * at + x) * block, block), block)
            for part in range(parts):
                turned = xs[2 * layer[label] + x, part].T
                xt[part * span : (part + 1) * span, lanes] = turned

    squares = []

    def own_block(phase, far, label):
        y = 1 - py if far else py
        both = pl.ds(2 * layer[label], 2)
        return gs[both, y, halves(phase)].reshape(2 * block, width)

    def other_block(label):
        return go[pl.ds(2 * layer[label], 2)].reshape(2 * block, width)

    def gradients(phase, fars, tiles, labels, events):
        tile = features // tiles
        first, final = labels[0] == LAYERS[0], labels[-1] == LAYERS[-1]
        start_token = LAYERS.index(labels[0]) * 2 * block
        tokens = slice(start_token, start_token + len(labels) * 2 * block)
        if phase == 2:
            for label in labels:
                for x in range(2):
                    shard = 2 * layer[label] + x
                    guarded(
                        px != x if label == "A" else None,
                        lambda shard=shard: landed(go.at[shard], o_sem.at[shard]),
                    )

        def body(step, total):
            rows = pl.ds(pl.multiple_of(step * tile, tile), tile)
            for far in fars:
                at = 4 if far == 2 else 2 * (phase - 2) + far
                right = jnp.concatenate(
                    [other_block(k) if far == 2 else own_block(phase, far, k) for k in labels], axis=0
                )
                value = wide_dot(xt[rows, tokens], right, ((1,), (0,)))
                if not first:
                    value = value + acc[at, rows, :]
                if final:
                    grad[rows, at * width : (at + 1) * width] = to_bf16(value)
                    if far < 2:
                        squared = (value * value).reshape(tile // 8, 8, width)
                        total = total + jnp.sum(squared, axis=0)
                else:
                    acc[at, rows, :] = value
            for number, names in enumerate(events):
                if names:

                    @pl.when(step == number)
                    def _(names=names):
                        for name in names:
                            travel(name)

            return total

        total = lax.fori_loop(0, features // tile, body, jnp.zeros((8, width), f32))
        if final:
            squares.append(total)

    mine = pl.ds(pl.multiple_of(fs * chunk, chunk), chunk)
    hidden = parts * width
    size = float(features * hidden)

    def outer_step(lanes, first, final):
        wide = 2 * chunk
        if final:
            square = jnp.sum(squares[0], axis=(0, 1), keepdims=True)
            for more in squares[1:]:
                square = square + jnp.sum(more, axis=(0, 1), keepdims=True)
            norms[0] = jnp.broadcast_to(square, norms.shape[1:])
            scale = (1.0 - stat_decay) / hidden * (size / (square + 1.0))
            swap_norm = pltpu.make_async_remote_copy(
                src_ref=norms.at[0], dst_ref=norms.at[1],
                send_sem=swap_sem.at[0], recv_sem=swap_sem.at[1],
                device_id=beside["core"], device_id_type=MESH,
            )
        if not final:

            broad = 2 * wide

            @pl.loop(0, features // broad)
            def _(step):
                rows = pl.ds(pl.multiple_of(step * broad, broad), broad)
                product = wide_dot(grad[mine, lanes], grad[rows, lanes], ((1,), (1,)))
                if not first:
                    product = product + sacc[:, rows]
                sacc[:, rows] = product

            return
        for step in range(features // wide):
            rows = slice(step * wide, (step + 1) * wide)
            product = wide_dot(grad[mine, lanes], grad[rows, lanes], ((1,), (1,)))
            s_ref[pc, :, rows] = to_bf16((product + sacc[:, rows]) * scale)
            if step == 0:
                swap_norm.start()
                dones.append(swap_norm)
            else:
                send_outer(step - 1)
        for load in loads[9:]:
            load.wait()
        send_outer(features // wide - 1)

    def outer_copy(which, step):
        rows = pl.ds(step * 2 * chunk, 2 * chunk)
        return pltpu.make_async_remote_copy(
            src_ref=s_ref.at[which, :, rows], dst_ref=s_ref.at[which, :, rows],
            send_sem=swap_sem.at[2 + step], recv_sem=swap_sem.at[6 + step],
            device_id=beside["core"], device_id_type=MESH,
        )

    def send_outer(step):
        outer_copy(pc, step).start()
        dones.append(step)

    def products(which, lanes):
        for step in range(features // chunk):
            rows = slice(step * chunk, (step + 1) * chunk)
            turn[:, rows] = grad[rows, lanes].T
        left = wide_dot(roots[which], grad[:, lanes], ((1,), (0,)))
        gram = wide_dot(turn[...], grad[:, lanes], ((1,), (0,)))
        for head in range(heads):
            at = slice(head * HEAD, (head + 1) * HEAD)
            k_ref[which, head] = gram[at, at]
            pre_ref[which, :, at] = wide_dot(
                to_bf16(left[:, at]), col_roots[which, head], ((1,), (0,))
            )

    def travel(op):
        phase = int(op[1])
        if op[0] == "w" or phase == 2:
            landed(*piece(phase, op[2:] or "Ac"))
        forward(phase, op[2:] or "Ac")

    for op in PROGRAM:
        kind, rest = op[0], op[1:]
        if isinstance(op, tuple):
            gradients(*BLOCKS[op[0][0]], op[0][1:], op[1:])
        elif kind in "ow":
            travel(op)
        elif kind == "C":
            cotangents()
        elif kind == "T":
            from_core(rest)
            transpose(rest)
        elif kind == "S":
            first, last = int(rest[0]), int(rest[1])
            outer_step(slice(first * width, (last + 1) * width), first == 0, last == 3)
        elif kind == "L":
            for load in loads[5:9]:
                load.wait()
        elif kind == "P":
            products(pc, slice(2 * width, 3 * width))
        elif kind == "Q":
            products(1 - pc, slice(4 * width, 5 * width))

    dones[0].wait()
    mine_sum, their_sum = norms[0, 0:1, 0:1], norms[1, 0:1, 0:1]
    sums = (
        jnp.where(pc == 0, mine_sum, their_sum),
        jnp.where(pc == 0, their_sum, mine_sum),
    )
    for which in range(2):
        scale_twice = size / (sums[which] + 1.0)
        pre_ref[which] = pre_ref[which] * jnp.sqrt(scale_twice)
        for head in range(heads):
            k_ref[which, head] = k_ref[which, head] * (
                (1.0 - stat_decay) / features * scale_twice
            )
    for cond, build in pending:
        guarded(cond, lambda build=build: build().wait_send())
    for step in dones[1:]:
        outer_copy(pc, step).wait_send()
        outer_copy(1 - pc, step).wait_recv()


def in_hbm(*arrays):
    return [pltpu.with_memory_space_constraint(array, pltpu.HBM) for array in arrays]


def relayed_products(x, query_grad, forget_grad, forget_pre, lower_bound, *held):
    shards, parts = lax.axis_size("fs"), lax.axis_size("tp")
    block, span = x.shape
    width = query_grad.shape[1]
    chunk, features = held[0].shape
    bf16, f32 = jnp.bfloat16, jnp.float32
    heads = held[2].shape
    vmem = pl.BlockSpec(memory_space=pltpu.VMEM)
    hbm = pl.BlockSpec(memory_space=pltpu.HBM)
    return pl.pallas_call(
        relay_kernel,
        out_shape=[
            pltpu.VMEM((2, chunk, features), bf16),
            pltpu.VMEM((2, chunk, width), f32),
            pltpu.VMEM((2,) + heads, f32),
            pltpu.VMEM((2, chunk, width), f32),
            pltpu.VMEM((2, chunk, width), f32),
            pltpu.VMEM((2, chunk, features), f32),
            pltpu.VMEM((2,) + heads, f32),
        ],
        in_specs=[hbm] * 17,
        out_specs=[vmem] * 7,
        scratch_shapes=[
            pltpu.VMEM((shards, parts, block, span), bf16),
            pltpu.VMEM((shards, 2, 2, block, width), bf16),
            pltpu.VMEM((shards, block, width), bf16),
            pltpu.VMEM((features, shards * block), bf16),
            pltpu.VMEM((parts + 1, features, width), f32),
            pltpu.VMEM((features, (parts + 1) * width), bf16),
            pltpu.VMEM((chunk, features), f32),
            pltpu.VMEM((2, 8, 128), f32),
            pltpu.VMEM((2, chunk, features), bf16),
            pltpu.VMEM((2,) + heads, bf16),
            pltpu.VMEM((3, block, width), bf16),
            pltpu.VMEM((1, width), f32),
            pltpu.VMEM((width, features), bf16),
            pltpu.SemaphoreType.DMA((17,)),
            pltpu.SemaphoreType.DMA((128,)),
            pltpu.SemaphoreType.DMA((2, shards, parts)),
            pltpu.SemaphoreType.DMA((2, shards, 2)),
            pltpu.SemaphoreType.DMA((shards,)),
            pltpu.SemaphoreType.DMA((10,)),
        ],
        compiler_params=pltpu.CompilerParams(
            collective_id=0, has_side_effects=True, vmem_limit_bytes=48 * 1024 * 1024
        ),
    )(
        *in_hbm(x, query_grad, forget_grad, forget_pre, lower_bound.reshape(1, -1), *held)
    )


def finish_kernel(outer_ref, pre_ref, column_ref, weight_ref, moment_ref, rows_ref, cols_ref, *outs):
    step = pl.program_id(0)
    tile, head_tile = outs[0].shape[0], outs[10].shape[1]
    at = pl.ds(pl.multiple_of(step * tile, tile), tile)
    head_at = pl.ds(pl.multiple_of(step * head_tile, head_tile), head_tile)
    for which in range(2):
        master_out, copy_out, step_out, moment_out, rows_out, cols_out = outs[which::2]
        precond = pre_ref[which, at, :]
        moment_next = moment_decay * moment_ref[which, at, :] + (1.0 - moment_decay) * precond
        update_step = moment_decay * moment_next + (1.0 - moment_decay) * precond
        master = weight_ref[which, at, :] - learn_rate * update_step
        master_out[...] = master
        copy_out[...] = to_bf16(master)
        step_out[...] = update_step
        moment_out[...] = moment_next
        rows_out[...] = stat_decay * rows_ref[which, at, :] + outer_ref[which, at, :].astype(
            jnp.float32
        )
        cols_out[...] = (
            stat_decay * cols_ref[which, :, head_at, :] + column_ref[which, :, head_at, :]
        )


def finished(held):
    f32, bf16 = jnp.float32, jnp.bfloat16
    _, chunk, features = held[0].shape
    width = held[1].shape[2]
    heads = held[2].shape[1:]
    steps = 4
    tile = chunk // steps
    narrow = pl.BlockSpec((tile, width), lambda i: (i, 0))
    wide = pl.BlockSpec((tile, features), lambda i: (i, 0))
    head = pl.BlockSpec((heads[0], heads[1] // steps, heads[2]), lambda i: (0, i, 0))
    flat = lambda kind: [jax.ShapeDtypeStruct((chunk, width), kind)] * 2
    return pl.pallas_call(
        finish_kernel,
        grid=(steps,),
        out_shape=flat(f32)
        + flat(bf16)
        + flat(f32)
        + flat(f32)
        + [jax.ShapeDtypeStruct((chunk, features), f32)] * 2
        + [jax.ShapeDtypeStruct(heads, f32)] * 2,
        in_specs=[pl.BlockSpec(memory_space=pltpu.VMEM)] * 7,
        out_specs=[narrow] * 8 + [wide] * 2 + [head] * 2,
        compiler_params=pltpu.CompilerParams(vmem_limit_bytes=24 * 1024 * 1024),
    )(*[pltpu.with_memory_space_constraint(array, pltpu.VMEM) for array in held])


def gather_plan(
    inputs,
    query_grad,
    forget_grad,
    forget_pre,
    lower_bound,
    query_weight,
    forget_weight,
    query_moment,
    forget_moment,
    query_rows,
    forget_rows,
    query_cols,
    forget_cols,
    query_row_root,
    forget_row_root,
    query_col_root,
    forget_col_root,
):
    held = relayed_products(
        inputs,
        query_grad,
        forget_grad,
        forget_pre,
        lower_bound,
        query_row_root,
        forget_row_root,
        query_col_root,
        forget_col_root,
        query_weight,
        forget_weight,
        query_moment,
        forget_moment,
        query_rows,
        forget_rows,
        query_cols,
        forget_cols,
    )
    return tuple(finished(held))


def on_device(*args):
    token_count = args[0].shape[0] * lax.axis_size("fs")
    feature_count = args[0].shape[1] * lax.axis_size("tp")
    paired = lax.axis_size("fs") == 8 and lax.axis_size("tp") == 4
    if paired and token_count <= feature_count:
        return gather_plan(*args)
    return reduce_plan(*args)


def solution(mesh):
    in_specs = (
        P("fs", "tp"),
        P("fs", "tp"),
        P("fs", "tp"),
        P("fs", "tp"),
        P("tp"),
        P("fs", "tp"),
        P("fs", "tp"),
        P("fs", "tp"),
        P("fs", "tp"),
        P("fs", None),
        P("fs", None),
        P("tp", None, None),
        P("tp", None, None),
        P("fs", None),
        P("fs", None),
        P("tp", None, None),
        P("tp", None, None),
    )
    out_specs = (
        P("fs", "tp"),
        P("fs", "tp"),
        P("fs", "tp"),
        P("fs", "tp"),
        P("fs", "tp"),
        P("fs", "tp"),
        P("fs", "tp"),
        P("fs", "tp"),
        P("fs", None),
        P("fs", None),
        P("tp", None, None),
        P("tp", None, None),
    )
    return jax.shard_map(
        on_device, mesh=mesh, in_specs=in_specs, out_specs=out_specs, check_vma=False
    )
```
